32 devices in a mesh: ep: 4 (over y, x), tp: 8 (over z, core).
Axes of the slice: x: 2, y: 2, z: 4, core: 2. Of those that a mesh axis runs over, the one named last changes fastest.
Arguments:
- queries: bfloat16 [2048, 16, 128], P('ep', 'tp'), may hold values from -300 to 300
- keys: bfloat16 [2048, 16, 128], P('ep', 'tp'), may hold values from -4 to 4
- values: bfloat16 [2048, 16, 128], P('ep', 'tp'), may hold values from -6 to 6
- mix_weight: float32 [16], P('tp'), may hold values from 0.3 to 0.8
- sub_gain: float32 [128], replicated, may hold values from 0.1 to 1.9
- tokens: bfloat16 [1024, 2048], P('ep', 'tp'), may hold values from -6 to 6
- routes: int32 [1024, 2], P('ep'), may hold values from 0 to 7, all different within a row; in each aligned block of 256 rows (0 to 255, 256 to 511, ...) at most 96 rows name the same one
- route_weights: float32 [1024, 2], P('ep'), may hold values from 0.1 to 1
- expert_gain: float32 [2048], replicated, may hold values from 0.1 to 1.9
- gate_weight: bfloat16 [8, 2048, 4096], P('ep', None, 'tp'), may hold values from -0.375 to 0.375
- up_weight: bfloat16 [8, 2048, 4096], P('ep', None, 'tp'), may hold values from -0.375 to 0.375
- down_weight: bfloat16 [8, 4096, 2048], P('ep', 'tp'), may hold values from -0.09375 to 0.09375
Outputs:
- attn_out: bfloat16 [2048, 16, 128], P('ep', 'tp')
- moe_out: bfloat16 [1024, 2048], P('ep', 'tp')
The draws below stay inside these ranges and needn't reach their ends.
Inputs may be any that keep to these rules, and one draw needn't show every extreme that they name: `routes`: in each aligned block of 256 rows no expert is named by more than 96 rows, and in every draw some expert is named by exactly 96 rows of some block.
All inputs are finite; a program needn't handle non-finite values.
Results may differ from the reference program's by a relative error of at most 0.018.
Values may be sent and summed in bfloat16 or wider, within the bound.
A program may use at most 128 MiB of HBM per device.

```python
import math
import jax
import jax.numpy as jnp
import numpy as np
from jax import lax

D = 2048
HEADS = 16
HEAD_QK = 64
HEAD_V = 128
FF = 4096
TOPK = 2
ROWS2 = 256
LENGTH = 2048
TOKENS2 = 1024
EXPERTS = 8
CAP = 96
N_EP = 4
N_TP = 8


def paired_fields(key):
    base = jax.random.fold_in(key, 31)
    query_key, field_key = jax.random.split(base, 2)
    shape = (LENGTH, HEADS, 2, HEAD_QK)
    queries = 1.8 * jax.random.truncated_normal(query_key, -4.0, 4.0, shape, jnp.float32)
    keys = jax.random.truncated_normal(field_key, -4.0, 4.0, shape, jnp.float32)
    return (queries.reshape(LENGTH, HEADS, 2 * HEAD_QK), keys.reshape(LENGTH, HEADS, 2 * HEAD_QK))


def draw_queries(key, part):
    return paired_fields(key)[0].astype(jnp.bfloat16)


def draw_keys(key, part):
    return paired_fields(key)[1].astype(jnp.bfloat16)


def block_scale(rng, dims, cuts, smallest, largest):
    def one(axis_at, shards_of):
        draws = jax.random.uniform(jax.random.fold_in(jax.random.fold_in(rng, 6), axis_at), (shards_of,), jnp.float32, smallest / len(cuts), largest / len(cuts))
        return jnp.repeat(jnp.exp(draws), dims[axis_at] // shards_of).reshape((-1,) + (1,) * (len(dims) - axis_at - 1))

    factor_of = one(*cuts[0])
    for cut in cuts[1:]:
        factor_of = factor_of * one(*cut)
    return factor_of


def assign_block(stream_key, own, number, rows, number_of, top, limit, lean):
    order = jax.random.permutation(stream_key, number_of)
    heavy_load, usual = shares(number_of, rows * top, limit, lean, True), shares(number_of, rows * top, limit, lean, False)
    places = jnp.arange(number_of)

    def named(sizes, offset_by):
        used = int((sizes > 0).sum())
        fixed = max(1, used // 4)
        moved = fixed + (places - fixed + offset_by * (used - fixed)) % max(1, number_of - fixed)
        return jnp.zeros((number_of,), jnp.int32).at[order[jnp.where(places < fixed, places, moved)]].set(jnp.asarray(sizes, jnp.int32))

    sizes = jnp.where(number % 4 == 0, named(heavy_load, number // 4), named(usual, number - number // 4 - 1))
    mixed = jax.random.permutation(jax.random.fold_in(own, 3), number_of)
    source_of, sink = mixed[0:number_of // 2 * 2:2], mixed[1:number_of // 2 * 2:2]
    margin = jnp.minimum(sizes[source_of] - 1, limit - sizes[sink]) // 2
    margin = jnp.where((source_of == order[0]) | (sink == order[0]) | (sizes[sink] == 0), 0, jnp.maximum(margin, 0))
    moved = jax.random.randint(jax.random.fold_in(own, 4), (number_of // 2,), 0, 1 << 20) % (margin + 1)
    sizes = sizes.at[source_of].add(-moved).at[sink].add(moved)
    labels = jnp.searchsorted(jnp.cumsum(sizes), jnp.arange(rows * top), side="right").astype(jnp.int32)
    listing = labels.reshape(top, rows).T
    listing = listing[jax.random.permutation(jax.random.fold_in(own, 1), rows)]
    offset_by = jax.random.randint(jax.random.fold_in(own, 2), (rows, 1), 0, top)
    return jnp.take_along_axis(listing, (jnp.arange(top)[None, :] + offset_by) % top, axis=1)


def shares(number_of, total, most, slope, full):
    loads = [(1 << 20) // math.isqrt(grade ** slope) + 1 for grade in range(1, number_of + 1)]
    largest = most if full else min(most, max(-(-total // number_of), total * loads[0] // sum(loads)))
    least = 1 if total - largest >= number_of - 1 else 0
    counts, surplus = [largest] + [least] * (number_of - 1), total - largest - least * (number_of - 1)
    while surplus > 0:
        movable = [i for i in range(1, number_of) if counts[i] < largest] or [i for i in range(1, number_of) if counts[i] < most]
        pool, remaining = sum([loads[i] for i in movable]), surplus
        for i in movable:
            extra = min(most - counts[i], max(1, remaining * loads[i] // pool), surplus)
            counts[i] = counts[i] + extra
            surplus = surplus - extra
    return np.array(counts)


def bell_draw(key, extent, width, bound, pieces=(), kind=jnp.bfloat16):
    entries = jax.random.normal(key, extent, jnp.float32) * width
    if len(pieces) > 0:
        entries = block_scale(key, extent, pieces, -0.22, 0.18) * entries
    return jnp.clip(entries, min=-bound, max=bound).astype(kind)


def setup_inputs(seed: int = 0) -> dict:
    arg_keys = jax.random.split(jax.random.key(seed), 13)
    queries = draw_queries(jax.random.fold_in(arg_keys[12], 71), 0)
    keys = draw_keys(jax.random.fold_in(arg_keys[12], 71), 0)
    values = bell_draw(arg_keys[2], (LENGTH, HEADS, HEAD_V), 1.0, 6.0, ((0, 4), (1, 8)))
    mix_weight = jnp.clip(0.3 + 0.5 * jax.random.uniform(arg_keys[3], (HEADS,), jnp.float32) ** block_scale(arg_keys[3], (HEADS,), ((0, 8),), -0.2, 0.2), 0.3, 0.8)
    sub_gain = jnp.clip(1.0 + 0.18 * jax.random.normal(arg_keys[4], (HEAD_V,), jnp.float32), 0.1, 1.9)
    tokens = bell_draw(arg_keys[5], (TOKENS2, D), 1.0, 6.0, ((0, 4), (1, 8)))
    routes_keys = jax.random.split(jax.random.fold_in(arg_keys[6], 1), TOKENS2 // ROWS2)
    routes_turns = jax.random.permutation(jax.random.fold_in(arg_keys[6], 3), TOKENS2 // ROWS2)
    routes = jax.vmap(lambda own, number: assign_block(jax.random.fold_in(arg_keys[6], 2), own, number, ROWS2, EXPERTS, TOPK, CAP, 1))(routes_keys, routes_turns).reshape((TOKENS2, TOPK))
    route_weights = jnp.clip(0.1 + 0.9 * jax.random.uniform(arg_keys[7], (TOKENS2, TOPK), jnp.float32) ** block_scale(arg_keys[7], (TOKENS2, TOPK), ((0, 4),), -0.2, 0.2), 0.1, 1.0)
    expert_gain = jnp.clip(1.0 + 0.18 * jax.random.normal(arg_keys[8], (D,), jnp.float32), 0.1, 1.9)
    gate_weight = bell_draw(arg_keys[9], (EXPERTS, D, FF), (D // 9) ** -0.5, 0.375, ((0, 4), (2, 8)))
    up_weight = bell_draw(arg_keys[10], (EXPERTS, D, FF), (D // 9) ** -0.5, 0.375, ((0, 4), (2, 8)))
    down_weight = bell_draw(arg_keys[11], (EXPERTS, FF, D), FF ** -0.5, 0.09375, ((0, 4), (1, 8)))
    return {"queries": queries, "keys": keys, "values": values, "mix_weight": mix_weight, "sub_gain": sub_gain, "tokens": tokens, "routes": routes, "route_weights": route_weights, "expert_gain": expert_gain, "gate_weight": gate_weight, "up_weight": up_weight, "down_weight": down_weight}


NEG_FILL = -1e+30
SUB_EPS = 1e-05
NORM_EPS = 1e-06
CLAMP_LIMIT = 7.0
GLU_ALPHA = 1.702
OUT_SCALE = 0.8

def head_attention(bundle, sub_gain):
    head_queries, head_keys, head_values, mix_value = bundle
    block_size = math.gcd(LENGTH, 512)
    key_all = head_keys.reshape(LENGTH, 2, HEAD_QK).astype(jnp.float32)
    key_pos = jnp.arange(LENGTH, dtype=jnp.int32)

    def one_block(block_index):
        offset = block_index * block_size
        query_block = lax.dynamic_slice_in_dim(head_queries, offset, block_size, 0)
        query_block = query_block.reshape(block_size, 2, HEAD_QK).astype(jnp.float32)
        scores = jnp.einsum('qmd,kmd->mqk', query_block, key_all) * HEAD_QK ** (-0.5)
        query_pos = offset + jnp.arange(block_size, dtype=jnp.int32)
        visible = key_pos[None, :] <= query_pos[:, None]
        row_max = lax.optimization_barrier(jnp.max(jnp.where(visible, scores, NEG_FILL), axis=-1))
        weights = jnp.where(visible, jnp.exp(scores - row_max[..., None]), 0.0)
        row_sum = lax.optimization_barrier(jnp.sum(weights, axis=-1))
        rounded = weights.astype(jnp.bfloat16)
        first = jnp.dot(rounded[0], head_values, preferred_element_type=jnp.float32) / row_sum[0][:, None]
        second = jnp.dot(rounded[1], head_values, preferred_element_type=jnp.float32) / row_sum[1][:, None]
        blend = first - mix_value * second
        scaled = blend * lax.rsqrt(lax.optimization_barrier(jnp.mean(blend * blend, axis=-1, keepdims=True)) + SUB_EPS)
        return (scaled * sub_gain * OUT_SCALE).astype(jnp.bfloat16)
    outputs = lax.map(one_block, jnp.arange(LENGTH // block_size, dtype=jnp.int32))
    return outputs.reshape(LENGTH, HEAD_V)

def reference(queries, keys, values, mix_weight, sub_gain, tokens, routes, route_weights, expert_gain, gate_weight, up_weight, down_weight):

    def per_head(bundle):
        return head_attention(bundle, sub_gain)
    heads_all = lax.map(per_head, (jnp.transpose(queries, (1, 0, 2)), jnp.transpose(keys, (1, 0, 2)), jnp.transpose(values, (1, 0, 2)), mix_weight))
    attn_out = jnp.transpose(heads_all, (1, 0, 2))
    floats = tokens.astype(jnp.float32)
    factor = lax.rsqrt(lax.optimization_barrier(jnp.mean(floats * floats, axis=-1)) + NORM_EPS)
    normed = (floats * expert_gain).astype(jnp.bfloat16)
    block_routes = routes.reshape(N_EP, ROWS2 * TOPK)
    onehot = (block_routes[..., None] == jnp.arange(EXPERTS, dtype=jnp.int32)[None, None, :]).astype(jnp.int32)
    slot_rank = lax.optimization_barrier(jnp.sum((jnp.cumsum(onehot, axis=1) - 1) * onehot, axis=2)).astype(jnp.int32)
    target = block_routes * CAP + slot_rank
    token_ids = (jnp.arange(N_EP, dtype=jnp.int32)[:, None] * ROWS2 + jnp.arange(ROWS2 * TOPK, dtype=jnp.int32)[None, :] // TOPK).astype(jnp.int32)
    block_ids = jnp.broadcast_to(jnp.arange(N_EP, dtype=jnp.int32)[:, None], target.shape)
    slot_owner = jnp.full((N_EP, EXPERTS * CAP), TOKENS2, jnp.int32).at[block_ids, target].set(token_ids)
    slot_owner = jnp.transpose(slot_owner.reshape(N_EP, EXPERTS, CAP), (1, 0, 2)).reshape(EXPERTS, N_EP * CAP)
    padded_rows = jnp.concatenate([normed, jnp.zeros((1, D), jnp.bfloat16)], axis=0)
    padded_factor = jnp.concatenate([factor, jnp.zeros((1,), jnp.float32)], axis=0)

    def run_expert(bundle):
        slot_list, expert_gate, expert_up, expert_down = bundle
        rows_in = padded_rows[slot_list]
        scale = padded_factor[slot_list][:, None]
        gate_pre = jnp.minimum(jnp.dot(rows_in, expert_gate, preferred_element_type=jnp.float32) * scale, CLAMP_LIMIT)
        up_pre = jnp.clip(jnp.dot(rows_in, expert_up, preferred_element_type=jnp.float32) * scale, -CLAMP_LIMIT, CLAMP_LIMIT)
        hidden = ((up_pre + 1.0) * gate_pre * jax.nn.sigmoid(GLU_ALPHA * gate_pre)).astype(jnp.bfloat16)
        hidden_parts = hidden.reshape(N_EP * CAP, N_TP, FF // N_TP)
        down_parts = expert_down.reshape(N_TP, FF // N_TP, D)

        def add_part(part_index, running):
            piece = jnp.dot(hidden_parts[:, part_index], down_parts[part_index], preferred_element_type=jnp.float32).astype(jnp.bfloat16)
            piece = lax.optimization_barrier(piece)
            return running + piece.astype(jnp.float32)
        summed = lax.fori_loop(0, N_TP, add_part, jnp.zeros((N_EP * CAP, D), jnp.float32))
        return summed.astype(jnp.bfloat16)
    expert_rows = lax.map(run_expert, (slot_owner, gate_weight, up_weight, down_weight)).reshape(EXPERTS, N_EP, CAP, D)
    row_block = (jnp.arange(TOKENS2, dtype=jnp.int32) // ROWS2)[:, None]
    picked = expert_rows[routes, jnp.broadcast_to(row_block, routes.shape), slot_rank.reshape(TOKENS2, TOPK)]
    moe_out = lax.optimization_barrier(jnp.sum(picked.astype(jnp.float32) * route_weights[..., None], axis=1)).astype(jnp.bfloat16)
    return (attn_out, moe_out)
```

```python
import functools

import jax
import jax.numpy as jnp
from jax import lax
from jax.experimental import pallas as pl
from jax.experimental.pallas import tpu as pltpu
from jax.sharding import PartitionSpec as P

NEG_FILL = -1e30
SUB_EPS = 1e-05
NORM_EPS = 1e-06
CLAMP_LIMIT = 7.0
GLU_ALPHA = 1.702
OUT_SCALE = 0.8
CORES = 2
F32 = jnp.float32
BF16 = jnp.bfloat16
MESH = pl.DeviceIdType.MESH


def dot(a, b):
    return jnp.dot(a, b, preferred_element_type=F32)


def dot_t(a, b):
    return lax.dot_general(a, b, (((1,), (1,)), ((), ())), preferred_element_type=F32)


def loop(lower, upper, body):
    def step(index, carry):
        body(index)
        return carry

    lax.fori_loop(lower, upper, step, 0)


def layer_kernel(
    n_ep, n_tp, cap, heads, rank_pad,
    tok_hbm, routes_hbm, route_w_hbm, gain_hbm, gate_hbm, up_hbm, down_hbm,
    q_hbm, k_hbm, v_hbm, sub_gain_hbm, mix,
    attn_out, moe_out,
    tok, routes_t, route_w_t, gain, q_in, k_in, v_in, sub_gain,
    gate, up, down, held, outgoing, arrived, normed, squares, gate_sum, up_sum, hidden, part, pair,
    fin, ex, slot_got, tok_stage, tok_got, held_sum, final, back, pick, pick_w, q, kv, kv_all,
    top, norm_sum, weighted,
    in_sem, w_sem, ag_s, ag_r, dp_s, dp_r, fw_s, fw_r, kv_s, kv_r, kh_s, kh_r, pr_s, pr_r,
    ex_s, ex_r, sl_s, sl_r, tk_s, tk_r, rt_s, rt_r,
):
    e, t = lax.axis_index("ep"), lax.axis_index("tp")
    nz = n_tp // CORES
    z, c = t // CORES, t % CORES
    partner = t + 1 - 2 * c
    rows, shard = tok.shape
    local = gate_hbm.shape[0]
    experts = n_ep * local
    pad = rank_pad
    slots = experts * pad
    block = local * pad
    has_up, has_dn = z < nz - 1, z > 0

    loads = [
        pltpu.make_async_copy(source, target, in_sem.at[i])
        for i, (source, target) in enumerate((
            (tok_hbm, tok), (routes_hbm, routes_t), (route_w_hbm, route_w_t), (gain_hbm, gain),
            (q_hbm, q_in), (k_hbm, k_in), (v_hbm, v_in), (sub_gain_hbm, sub_gain)))
    ]
    for copy in loads:
        copy.start()
    weights = [
        pltpu.make_async_copy(source, target, w_sem.at[i])
        for i, (source, target) in enumerate(((gate_hbm, gate), (up_hbm, up), (down_hbm, down)))
    ]
    for copy in weights:
        copy.start()

    barrier = pltpu.get_barrier_semaphore()
    pl.semaphore_signal(barrier, inc=1, device_id=(e, partner), device_id_type=MESH)

    @pl.when(has_up)
    def _():
        pl.semaphore_signal(barrier, inc=1, device_id=(e, t + CORES), device_id_type=MESH)

    @pl.when(has_dn)
    def _():
        pl.semaphore_signal(barrier, inc=1, device_id=(e, t - CORES), device_id_type=MESH)

    loop(1, n_ep, lambda d: pl.semaphore_signal(
        barrier, inc=1, device_id=((e + d) % n_ep, t), device_id_type=MESH))
    for copy in loads[:2]:
        copy.wait()
    with jax.named_scope("barrier"):
        pl.semaphore_wait(barrier, n_ep + has_up.astype(jnp.int32) + has_dn.astype(jnp.int32))

    def send(source, target, s_sem, r_sem, device):
        return pltpu.make_async_remote_copy(
            src_ref=source, dst_ref=target, send_sem=s_sem, recv_sem=r_sem,
            device_id=device, device_id_type=MESH)

    def shard_copy(way, r, origin):
        source = tok if r == 0 else held.at[origin]
        target = t + CORES if way == 0 else t - CORES
        return send(source, held.at[origin], ag_s.at[way, r], ag_r.at[way, r], (e, target))

    def shard_sends(r):
        @pl.when(has_up & (z - r >= 0))
        def _():
            shard_copy(0, r, z - r).start()

        @pl.when(has_dn & (z + r < nz))
        def _():
            shard_copy(1, r, z + r).start()

    def shard_send_waits(r):
        @pl.when(has_up & (z - r >= 0))
        def _():
            shard_copy(0, r, z - r).wait_send()

        @pl.when(has_dn & (z + r < nz))
        def _():
            shard_copy(1, r, z + r).wait_send()

    shard_sends(0)

    row_i = lax.broadcasted_iota(jnp.int32, (rows, rows), 0)
    col_i = lax.broadcasted_iota(jnp.int32, (rows, rows), 1)
    picks = routes_t.shape[0]
    exp_row = lax.broadcasted_iota(jnp.int32, (experts, rows), 0)
    hot_t = [(routes_t[p:p + 1, :] == exp_row).astype(F32) for p in range(picks)]
    before_t = dot(sum(hot_t).astype(BF16), (row_i < col_i).astype(F32).astype(BF16))
    slot_row = [
        jnp.sum(h * (before_t + (exp_row * pad).astype(F32)), axis=0, keepdims=True)
        for h in hot_t
    ]
    slot_i = lax.broadcasted_iota(jnp.int32, (slots, rows), 0).astype(F32)

    def as_column(line):
        return jnp.transpose(jnp.broadcast_to(line, (128, rows)))[:, :1]

    choose = sum((slot_i == s).astype(F32) for s in slot_row).astype(BF16)

    def piece(k, d):
        source = outgoing.at[k, (e + d) % n_ep]
        return send(source, arrived.at[CORES * k + c, e], dp_s.at[k, d - 1], dp_r.at[k, d - 1],
                    ((e + d) % n_ep, t))

    def incoming(k, d):
        origin = (e + n_ep - d) % n_ep
        return send(outgoing.at[k, origin], arrived.at[CORES * k + c, origin],
                    dp_s.at[k, d - 1], dp_r.at[k, d - 1], (origin, t))

    def forward(k, d):
        origin = (e + n_ep - d) % n_ep
        place = arrived.at[CORES * k + c, origin]
        return send(place, place, fw_s.at[k, d], fw_r.at[k, d], (e, partner))

    def forwarded(k, d):
        origin = (e + n_ep - d) % n_ep
        place = arrived.at[CORES * k + 1 - c, origin]
        return send(place, place, fw_s.at[k, d], fw_r.at[k, d], (e, partner))

    def dispatch(k, source):
        made = dot(choose, source).astype(BF16).reshape(n_ep, block, shard)
        outgoing[k] = made
        arrived[CORES * k + c, e] = outgoing[k, e]
        loop(1, n_ep, lambda d: piece(k, d).start())
        forward(k, 0).start()

    items = q.shape[1]

    def unpack():
        for copy in loads[2:]:
            copy.wait()
        pick_i = lax.broadcasted_iota(jnp.int32, (items, items * heads), 0)
        from_i = lax.broadcasted_iota(jnp.int32, (items, items * heads), 1)
        for h in range(heads):
            take = (from_i == pick_i * heads + h).astype(F32).astype(BF16)
            q[h] = dot(take, q_in[...]).astype(BF16)
            kv[0, h] = dot(take, k_in[...]).astype(BF16)
            kv[1, h] = dot(take, v_in[...]).astype(BF16)

    def pick_tables():
        lane_slot = lax.broadcasted_iota(jnp.int32, (rows, slots), 1).astype(F32)
        for p in range(picks):
            pick[p] = (lane_slot == as_column(slot_row[p])).astype(F32).astype(BF16)
            pick_w[p] = jnp.transpose(jnp.broadcast_to(route_w_t[p:p + 1, :], (128, rows)))

    length, width = q.shape[1:]
    lane = lax.broadcasted_iota(jnp.int32, (length, width), 1)
    scale = (width // 2) ** -0.5

    def attend(keys_values, diagonal):
        for h in range(heads):
            key, value = keys_values[0, h], keys_values[1, h]
            scaled_q = q[h].astype(F32) * scale
            for m in range(2):
                n = 2 * h + m
                mine = (lane < width // 2) if m == 0 else (lane >= width // 2)
                query = jnp.where(mine, scaled_q, 0.0).astype(BF16)
                scores = dot_t(query, key)
                if diagonal:
                    q_pos = lax.broadcasted_iota(jnp.int32, scores.shape, 0)
                    k_pos = lax.broadcasted_iota(jnp.int32, scores.shape, 1)
                    scores = jnp.where(k_pos <= q_pos, scores, NEG_FILL)
                high = jnp.max(scores, axis=1, keepdims=True)
                if not diagonal:
                    old = top[n]
                    high = jnp.maximum(high, old)
                    shrink = jnp.exp(old - high)
                w = jnp.exp(scores - high)
                s = jnp.sum(w, axis=1, keepdims=True)
                v = dot(w.astype(BF16), value)
                top[n] = high
                norm_sum[n] = s if diagonal else norm_sum[n] * shrink + s
                weighted[n] = v if diagonal else weighted[n] * shrink + v

    relay = n_ep == 4

    def kv_copy(d):
        return send(kv, kv_all.at[e], kv_s.at[d - 1], kv_r.at[e], ((e + d) % n_ep, t))

    def kv_got(origin):
        return send(kv, kv_all.at[origin], kv_s.at[0], kv_r.at[origin], (origin, t))

    def kv_direct(d, action):
        if relay and d == 1:
            @pl.when(e % 2 == 0)
            def _():
                action(kv_copy(d))
        elif relay and d == 2:
            @pl.when(e < 2)
            def _():
                action(kv_copy(d))
        elif not relay:
            @pl.when(e + d < n_ep)
            def _():
                action(kv_copy(d))

    def kv_half(origin, half, device):
        place = kv_all.at[origin, half]
        return send(place, place, kh_s.at[origin, half], kh_r.at[origin, half], (device, t))

    def kv_cross(action):
        if relay:
            @pl.when(e == 1)
            def _():
                action(send(kv.at[0], kv_all.at[1, 0], kh_s.at[1, 0], kh_r.at[1, 0], (2, t)))

    def kv_pass(origin, action):
        if relay:
            for half in range(2):
                @pl.when((e == half + 1) & (origin == 0))
                def _():
                    action(kv_half(0, half, 3))

            @pl.when((e == 3) & (origin == 1))
            def _():
                action(kv_half(1, 1, 2))

    def far_origin(j):
        if relay:
            return jnp.where(e == 3, (j + 1) % 3, j)
        return e - 1 - j

    def attend_far(lower, upper):
        def body(j):
            origin = far_origin(j)
            if relay:
                halves = ((e == 3) & (origin == 0)) | ((e == 2) & (origin == 1))

                @pl.when(halves)
                def _():
                    for half in range(2):
                        kv_half(origin, half, 3).wait_recv()

                @pl.when(jnp.logical_not(halves))
                def _():
                    kv_got(origin).wait_recv()
            else:
                kv_got(origin).wait_recv()
            kv_pass(origin, lambda copy: copy.start())
            attend(kv_all.at[origin], False)

        loop(lower, jnp.minimum(upper, e), body)

    with jax.named_scope("dispatch_own"):
        dispatch(z, tok[...])
    with jax.named_scope("unpack"):
        unpack()
    for r in range(nz - 1):
        got_up = has_dn & (z - 1 - r >= 0)
        got_dn = has_up & (z + 1 + r < nz)

        with jax.named_scope("shard_wait"):
            @pl.when(got_up)
            def _():
                shard_copy(0, r, z - 1 - r).wait_recv()

            @pl.when(got_dn)
            def _():
                shard_copy(1, r, z + 1 + r).wait_recv()

            if r < nz - 2:
                shard_sends(r + 1)

        with jax.named_scope("dispatch"):
            @pl.when(got_up)
            def _():
                dispatch(z - 1 - r, held[z - 1 - r])

            @pl.when(got_dn)
            def _():
                dispatch(z + 1 + r, held[z + 1 + r])

        if r == 0:
            with jax.named_scope("diag"):
                attend(kv, True)
    for d in range(1, n_ep):
        kv_direct(d, lambda copy: copy.start())
    kv_cross(lambda copy: copy.start())

    def pass_on(k):
        def body(d):
            incoming(k, d).wait_recv()
            forward(k, d).start()

        loop(1, n_ep, body)

    for copy in weights:
        copy.wait()
    gate_sum[...] = jnp.zeros_like(gate_sum)
    up_sum[...] = jnp.zeros_like(up_sum)
    squares[...] = jnp.zeros_like(squares)
    width_total = gain.shape[2] * n_tp
    deep = CORES * shard

    def absorb(k):
        loop(0, n_ep, lambda d: forwarded(k, d).wait_recv())

        def prepare(source):
            place = pl.ds(pl.multiple_of(source * pad, pad), pad)
            for x in range(local):
                for half in range(CORES):
                    floats = arrived[CORES * k + half, source, x * pad:(x + 1) * pad, :].astype(F32)
                    squares[x, place, :] += floats * floats
                    normed[x, place, half * shard:(half + 1) * shard] = (
                        floats * gain[CORES * k + half]).astype(BF16)

        loop(0, n_ep, prepare)
        depth = pl.ds(pl.multiple_of(k * deep, deep), deep)
        for x in range(local):
            gate_sum[x] += dot(normed[x], gate[x, depth, :])
            up_sum[x] += dot(normed[x], up[x, depth, :])

    def visit(i, action):
        k = z - (i + 1) // 2 * (i % 2) + i // 2 * (1 - i % 2)

        @pl.when((k >= 0) & (k < nz))
        def _():
            action(k)

    def arrival(i):
        @pl.when(i < 2 * nz - 1)
        def _():
            visit(i, pass_on)

        @pl.when(i >= 2)
        def _():
            visit(i - 2, absorb)

    with jax.named_scope("absorb"):
        loop(0, 2 * nz + 1, arrival)

    with jax.named_scope("picks"):
        pick_tables()

    count = n_ep * pad

    def goal(i):
        return jnp.where(2 * z < nz, nz - 1 - i, i)

    def pair_copy(k):
        return send(part.at[1 - c, k], pair.at[k], pr_s.at[k], pr_r.at[k], (e, partner))

    def exchange(k, d):
        target = (e + d) % n_ep
        return send(fin.at[k, target], ex.at[k, e], ex_s.at[k, d - 1], ex_r.at[k, d - 1], (target, t))

    def exchanged(k, d):
        origin = (e + n_ep - d) % n_ep
        return send(fin.at[k, origin], ex.at[k, origin], ex_s.at[k, d - 1], ex_r.at[k, d - 1],
                    (origin, t))

    def slot_copy(way):
        k = z + 1 if way == 0 else z - 1
        target = t + CORES if way == 0 else t - CORES
        return send(fin.at[k], slot_got.at[way], sl_s.at[way], sl_r.at[way], (e, target))

    def slot_recv(way):
        return send(fin.at[z], slot_got.at[way], sl_s.at[way], sl_r.at[way], (e, partner))

    def token_copy(k):
        return send(tok_stage.at[k], tok_got.at[z], tk_s.at[k], tk_r.at[z], (e, CORES * k + c))

    def token_got(k):
        return send(tok_stage.at[k], tok_got.at[k], tk_s.at[k], tk_r.at[k], (e, CORES * k + c))

    def is_far(k):
        return (k > z + 1) | (k < z - 1)

    with jax.named_scope("hidden"):
        for x in range(local):
            mean = jnp.sum(squares[x], axis=1, keepdims=True) / width_total
            factor = lax.rsqrt(mean + NORM_EPS)
            gate_pre = jnp.minimum(gate_sum[x] * factor, CLAMP_LIMIT)
            up_pre = jnp.clip(up_sum[x] * factor, -CLAMP_LIMIT, CLAMP_LIMIT)
            hidden[x] = ((up_pre + 1.0) * gate_pre * jax.nn.sigmoid(GLU_ALPHA * gate_pre)).astype(BF16)

    def project(i):
        k = goal(i)
        place = pl.ds(pl.multiple_of(k * deep, deep), deep)
        for x in range(local):
            product = dot(hidden[x], down[x, :, place]).astype(BF16)
            for half in range(CORES):
                part[half, k, x] = product[:, half * shard:(half + 1) * shard]
        pair_copy(k).start()

    def finish(i):
        k = goal(i)
        pair_copy(k).wait_recv()
        for x in range(local):
            both = (part[c, k, x].astype(F32) + pair[k, x].astype(F32)).astype(BF16)
            for source in range(n_ep):
                fin[k, source, x * pad:(x + 1) * pad, :] = both[source * pad:(source + 1) * pad, :]

        @pl.when(is_far(k))
        def _():
            loop(1, n_ep, lambda d: exchange(k, d).start())

        @pl.when(k == z + 1)
        def _():
            slot_copy(0).start()

        @pl.when(k == z - 1)
        def _():
            slot_copy(1).start()

    with jax.named_scope("project"):
        loop(0, nz, project)
    with jax.named_scope("finish"):
        loop(0, nz, finish)

    def mixture(results):
        mixed = None
        for p in range(picks):
            selected = dot(pick[p], results)
            weight = jnp.concatenate([pick_w[p]] * (shard // 128), axis=1)
            mixed = selected * weight if mixed is None else mixed + selected * weight
        return mixed

    def tokens_out(i):
        k = goal(i)

        @pl.when(is_far(k))
        def _():
            ex[k, e] = fin[k, e]
            loop(1, n_ep, lambda d: exchanged(k, d).wait_recv())
            tok_stage[k] = mixture(ex[k].reshape(slots, shard)).astype(BF16)
            token_copy(k).start()

    third = (n_ep - 1 + 2) // 3
    with jax.named_scope("far0"):
        attend_far(0, third)
    with jax.named_scope("tokens_out"):
        loop(0, nz, tokens_out)
    with jax.named_scope("slots_in"):
        @pl.when(has_dn)
        def _():
            slot_recv(0).wait_recv()

        @pl.when(has_up)
        def _():
            slot_recv(1).wait_recv()

        for x in range(local):
            span = slice(x * pad, (x + 1) * pad)
            for source in range(n_ep):
                total = fin[z, source, span, :].astype(F32)
                low = slot_got[0, source, span, :].astype(F32)
                high = slot_got[1, source, span, :].astype(F32)
                total = total + jnp.where(has_dn, low, 0.0) + jnp.where(has_up, high, 0.0)
                final[source, span, :] = total.astype(BF16)

    def give(d):
        return send(final.at[(e + d) % n_ep], back.at[e], rt_s.at[d - 1], rt_r.at[d - 1],
                    ((e + d) % n_ep, t))

    def given(d):
        origin = (e + n_ep - d) % n_ep
        return send(final.at[origin], back.at[origin], rt_s.at[d - 1], rt_r.at[d - 1], (origin, t))

    loop(1, n_ep, lambda d: give(d).start())
    back[e] = final[e]

    with jax.named_scope("far1"):
        attend_far(third, 2 * third)
    with jax.named_scope("far2"):
        attend_far(2 * third, n_ep)
    with jax.named_scope("attn_fin"):
        for h in range(heads):
            first = weighted[2 * h] / norm_sum[2 * h]
            second = weighted[2 * h + 1] / norm_sum[2 * h + 1]
            blend = first - mix[h] * second
            mean = jnp.mean(blend * blend, axis=1, keepdims=True)
            scaled = (blend * lax.rsqrt(mean + SUB_EPS) * sub_gain[...] * OUT_SCALE).astype(BF16)
            put_i = lax.broadcasted_iota(jnp.int32, (items * heads, items), 0)
            of_i = lax.broadcasted_iota(jnp.int32, (items * heads, items), 1)
            placed = dot((put_i == of_i * heads + h).astype(F32).astype(BF16), scaled)
            woven = placed if h == 0 else woven + placed
        attn_out[...] = woven.astype(BF16)

    with jax.named_scope("send_waits"):
        for r in range(nz - 1):
            shard_send_waits(r)
        loop(0, nz, lambda k: loop(1, n_ep, lambda d: piece(k, d).wait_send()))
        loop(0, nz, lambda k: loop(0, n_ep, lambda d: forward(k, d).wait_send()))
        for d in range(1, n_ep):
            kv_direct(d, lambda copy: copy.wait_send())
        kv_cross(lambda copy: copy.wait_send())
        if relay:
            for origin in range(2):
                kv_pass(origin, lambda copy: copy.wait_send())
        loop(0, nz, lambda k: pair_copy(k).wait_send())

        def far_waits(k):
            @pl.when(is_far(k))
            def _():
                loop(1, n_ep, lambda d: exchange(k, d).wait_send())
                token_copy(k).wait_send()

        loop(0, nz, far_waits)

        @pl.when(has_up)
        def _():
            slot_copy(0).wait_send()

        @pl.when(has_dn)
        def _():
            slot_copy(1).wait_send()

    with jax.named_scope("tokens_in"):
        held_sum[...] = jnp.zeros_like(held_sum)

        def add_far(k):
            @pl.when(is_far(k))
            def _():
                token_got(k).wait_recv()
                held_sum[...] += tok_got[k].astype(F32)

        loop(0, nz, add_far)

    with jax.named_scope("given_wait"):
        loop(1, n_ep, lambda d: given(d).wait_recv())
    with jax.named_scope("combine"):
        moe_out[...] = (mixture(back[...].reshape(slots, shard)) + held_sum[...]).astype(BF16)
        loop(1, n_ep, lambda d: give(d).wait_send())


def make_shards(n_ep, n_tp):
    def shards(
        queries, keys, values, mix_weight, sub_gain, tokens, routes, route_weights,
        expert_gain, gate_weight, up_weight, down_weight,
    ):
        rows, shard = tokens.shape
        picks = routes.shape[1]
        local, depth, units = gate_weight.shape
        cap = 3 * rows * picks // (2 * n_ep * local)
        pad = -(-cap // 16) * 16
        length, heads, width = queries.shape
        value_width = values.shape[2]
        nz = n_tp // CORES
        block = local * pad
        count = n_ep * pad
        vmem = pl.BlockSpec(memory_space=pltpu.VMEM)
        hbm = pl.BlockSpec(memory_space=pltpu.HBM)
        dma = pltpu.SemaphoreType.DMA
        peers = n_ep - 1
        attn, moe = pl.pallas_call(
            functools.partial(layer_kernel, n_ep, n_tp, cap, heads, pad),
            out_shape=(
                pltpu.VMEM((length * heads, value_width), BF16),
                pltpu.VMEM((rows, shard), BF16),
            ),
            in_specs=[hbm] * 11 + [pl.BlockSpec(memory_space=pltpu.SMEM)],
            out_specs=(vmem, vmem),
            scratch_shapes=[
                pltpu.VMEM((rows, shard), BF16),
                pltpu.VMEM((picks, rows), jnp.int32),
                pltpu.VMEM((picks, rows), F32),
                pltpu.VMEM((n_tp, 1, shard), F32),
                pltpu.VMEM((length * heads, width), BF16),
                pltpu.VMEM((length * heads, width), BF16),
                pltpu.VMEM((length * heads, value_width), BF16),
                pltpu.VMEM((1, value_width), F32),
                pltpu.VMEM(gate_weight.shape, BF16),
                pltpu.VMEM(up_weight.shape, BF16),
                pltpu.VMEM(down_weight.shape, BF16),
                pltpu.VMEM((nz, rows, shard), BF16),
                pltpu.VMEM((nz, n_ep, block, shard), BF16),
                pltpu.VMEM((n_tp, n_ep, block, shard), BF16),
                pltpu.VMEM((local, count, CORES * shard), BF16),
                pltpu.VMEM((local, count, shard), F32),
                pltpu.VMEM((local, count, units), F32),
                pltpu.VMEM((local, count, units), F32),
                pltpu.VMEM((local, count, units), BF16),
                pltpu.VMEM((CORES, nz, local, count, shard), BF16),
                pltpu.VMEM((nz, local, count, shard), BF16),
                pltpu.VMEM((nz, n_ep, block, shard), BF16),
                pltpu.VMEM((nz, n_ep, block, shard), BF16),
                pltpu.VMEM((2, n_ep, block, shard), BF16),
                pltpu.VMEM((nz, rows, shard), BF16),
                pltpu.VMEM((nz, rows, shard), BF16),
                pltpu.VMEM((rows, shard), F32),
                pltpu.VMEM((n_ep, block, shard), BF16),
                pltpu.VMEM((n_ep, block, shard), BF16),
                pltpu.VMEM((picks, rows, n_ep * block), BF16),
                pltpu.VMEM((picks, rows, 128), F32),
                pltpu.VMEM((heads, length, width), BF16),
                pltpu.VMEM((2, heads, length, width), BF16),
                pltpu.VMEM((n_ep, 2, heads, length, width), BF16),
                pltpu.VMEM((2 * heads, length, 1), F32),
                pltpu.VMEM((2 * heads, length, 1), F32),
                pltpu.VMEM((2 * heads, length, value_width), F32),
                dma((8,)),
                dma((3,)),
                dma((2, nz - 1)), dma((2, nz - 1)),
                dma((nz, peers)), dma((nz, peers)),
                dma((nz, n_ep)), dma((nz, n_ep)),
                dma((max(peers, 2),)), dma((n_ep,)),
                dma((2, 2)), dma((2, 2)),
                dma((nz,)), dma((nz,)),
                dma((nz, peers)), dma((nz, peers)),
                dma((2,)), dma((2,)),
                dma((nz,)), dma((nz,)),
                dma((peers,)), dma((peers,)),
            ],
            compiler_params=pltpu.CompilerParams(
                collective_id=0, has_side_effects=True, vmem_limit_bytes=54 * 2**20),
            name="layer",
        )(*(pltpu.with_memory_space_constraint(x, pltpu.HBM) for x in (
            tokens, jnp.transpose(routes), jnp.transpose(route_weights),
            expert_gain.reshape(n_tp, 1, shard), gate_weight, up_weight, down_weight,
            queries.reshape(length * heads, width), keys.reshape(length * heads, width),
            values.reshape(length * heads, value_width), sub_gain[None, :],
        )), mix_weight)
        return attn.reshape(length, heads, value_width), moe

    return shards


def solution(mesh):
    return jax.shard_map(
        make_shards(mesh.shape["ep"], mesh.shape["tp"]),
        mesh=mesh,
        in_specs=(
            P("ep", "tp", None),
            P("ep", "tp", None),
            P("ep", "tp", None),
            P("tp"),
            P(),
            P("ep", "tp"),
            P("ep", None),
            P("ep", None),
            P(),
            P("ep", None, "tp"),
            P("ep", None, "tp"),
            P("ep", "tp", None),
        ),
        out_specs=(P("ep", "tp", None), P("ep", "tp")),
        check_vma=False,
    )
```

```python
import functools

import jax
import jax.numpy as jnp
from jax import lax
from jax.experimental import pallas as pl
from jax.experimental.pallas import tpu as pltpu
from jax.sharding import PartitionSpec as P

NEG_FILL = -1e30
SUB_EPS = 1e-05
NORM_EPS = 1e-06
CLAMP_LIMIT = 7.0
GLU_ALPHA = 1.702
OUT_SCALE = 0.8
CORES = 2
LANES = 128
F32 = jnp.float32
BF16 = jnp.bfloat16
MESH = pl.DeviceIdType.MESH


def dot(a, b):
    return jnp.dot(a, b, preferred_element_type=F32)


def dot_t(a, b):
    return lax.dot_general(a, b, (((1,), (1,)), ((), ())), preferred_element_type=F32)


def loop(lower, upper, body):
    def step(index, carry):
        body(index)
        return carry

    lax.fori_loop(lower, upper, step, 0)


def layer_kernel(
    n_ep, n_tp, cap, heads, rank_pad,
    tok_hbm, routes_hbm, route_w_hbm, gain_hbm, gate_hbm, up_hbm, down_hbm,
    q_hbm, k_hbm, v_hbm, sub_gain_hbm, mix,
    attn_out, moe_out,
    tok, routes_t, route_w_t, gain, q_in, k_in, v_in, sub_gain,
    gate, up, down, held, outgoing, arrived, normed, squares, gate_sum, up_sum, hidden, part, pair,
    fin, ex, slot_got, tok_stage, tok_got, held_sum, final, back, pick, pick_w, q, kv, kv_all,
    top, norm_sum, weighted,
    in_sem, w_sem, ag_s, ag_r, dp_s, dp_r, fw_s, fw_r, kv_s, kv_r, kh_s, kh_r, pr_s, pr_r,
    ex_s, ex_r, sl_s, sl_r, tk_s, tk_r, rt_s, rt_r,
):
    e, t = lax.axis_index("ep"), lax.axis_index("tp")
    nz = n_tp // CORES
    z, c = t // CORES, t % CORES
    partner = t + 1 - 2 * c
    rows, shard = tok.shape
    local = gate_hbm.shape[0]
    experts = n_ep * local
    pad = rank_pad
    slots = experts * pad
    block = local * pad
    has_up, has_dn = z < nz - 1, z > 0

    loads = [
        pltpu.make_async_copy(source, target, in_sem.at[i])
        for i, (source, target) in enumerate((
            (tok_hbm, tok), (routes_hbm, routes_t), (route_w_hbm, route_w_t), (gain_hbm, gain),
            (q_hbm, q_in), (k_hbm, k_in), (v_hbm, v_in), (sub_gain_hbm, sub_gain)))
    ]
    for copy in loads:
        copy.start()
    weights = [
        pltpu.make_async_copy(source, target, w_sem.at[i])
        for i, (source, target) in enumerate(((gate_hbm, gate), (up_hbm, up), (down_hbm, down)))
    ]
    for copy in weights:
        copy.start()

    barrier = pltpu.get_barrier_semaphore()
    pl.semaphore_signal(barrier, inc=1, device_id=(e, partner), device_id_type=MESH)

    @pl.when(has_up)
    def _():
        pl.semaphore_signal(barrier, inc=1, device_id=(e, t + CORES), device_id_type=MESH)

    @pl.when(has_dn)
    def _():
        pl.semaphore_signal(barrier, inc=1, device_id=(e, t - CORES), device_id_type=MESH)

    loop(1, n_ep, lambda d: pl.semaphore_signal(
        barrier, inc=1, device_id=((e + d) % n_ep, t), device_id_type=MESH))
    for copy in loads[:2]:
        copy.wait()
    with jax.named_scope("barrier"):
        pl.semaphore_wait(barrier, n_ep + has_up.astype(jnp.int32) + has_dn.astype(jnp.int32))

    def send(source, target, s_sem, r_sem, device):
        return pltpu.make_async_remote_copy(
            src_ref=source, dst_ref=target, send_sem=s_sem, recv_sem=r_sem,
            device_id=device, device_id_type=MESH)

    def shard_copy(way, r, origin):
        source = tok if r == 0 else held.at[origin]
        target = t + CORES if way == 0 else t - CORES
        return send(source, held.at[origin], ag_s.at[way, r], ag_r.at[way, r], (e, target))

    def shard_sends(r):
        @pl.when(has_up & (z - r >= 0))
        def _():
            shard_copy(0, r, z - r).start()

        @pl.when(has_dn & (z + r < nz))
        def _():
            shard_copy(1, r, z + r).start()

    def shard_send_waits(r):
        @pl.when(has_up & (z - r >= 0))
        def _():
            shard_copy(0, r, z - r).wait_send()

        @pl.when(has_dn & (z + r < nz))
        def _():
            shard_copy(1, r, z + r).wait_send()

    shard_sends(0)

    row_i = lax.broadcasted_iota(jnp.int32, (rows, rows), 0)
    col_i = lax.broadcasted_iota(jnp.int32, (rows, rows), 1)
    picks = routes_t.shape[0]
    exp_row = lax.broadcasted_iota(jnp.int32, (experts, rows), 0)
    hot_t = [(routes_t[p:p + 1, :] == exp_row).astype(F32) for p in range(picks)]
    before_t = dot(sum(hot_t).astype(BF16), (row_i < col_i).astype(F32).astype(BF16))
    slot_row = [
        jnp.sum(h * (before_t + (exp_row * pad).astype(F32)), axis=0, keepdims=True)
        for h in hot_t
    ]
    slot_i = lax.broadcasted_iota(jnp.int32, (slots, rows), 0).astype(F32)

    def as_column(line):
        return jnp.transpose(jnp.broadcast_to(line, (128, rows)))[:, :1]

    choose = sum((slot_i == s).astype(F32) for s in slot_row).astype(BF16)

    def piece(k, d):
        source = outgoing.at[k, (e + d) % n_ep]
        return send(source, arrived.at[CORES * k + c, e], dp_s.at[k, d - 1], dp_r.at[k, d - 1],
                    ((e + d) % n_ep, t))

    def incoming(k, d):
        origin = (e + n_ep - d) % n_ep
        return send(outgoing.at[k, origin], arrived.at[CORES * k + c, origin],
                    dp_s.at[k, d - 1], dp_r.at[k, d - 1], (origin, t))

    def forward(k, d):
        origin = (e + n_ep - d) % n_ep
        place = arrived.at[CORES * k + c, origin]
        return send(place, place, fw_s.at[k, d], fw_r.at[k, d], (e, partner))

    def forwarded(k, d):
        origin = (e + n_ep - d) % n_ep
        place = arrived.at[CORES * k + 1 - c, origin]
        return send(place, place, fw_s.at[k, d], fw_r.at[k, d], (e, partner))

    def dispatch(k, source):
        made = dot(choose, source).astype(BF16).reshape(n_ep, block, shard)
        outgoing[k] = made
        arrived[CORES * k + c, e] = outgoing[k, e]
        loop(1, n_ep, lambda d: piece(k, d).start())
        forward(k, 0).start()

    items, width = q.shape[1:]

    def unpack():
        for copy in loads[2:]:
            copy.wait()
        pick_i = lax.broadcasted_iota(jnp.int32, (items, items * heads), 0)
        from_i = lax.broadcasted_iota(jnp.int32, (items, items * heads), 1)
        for h in range(heads):
            take = (from_i == pick_i * heads + h).astype(F32).astype(BF16)
            scaled_q = dot(take, q_in[...]) * (width // 2) ** -0.5
            lane = lax.broadcasted_iota(jnp.int32, (items, width), 1)
            for m in range(2):
                mine = (lane < width // 2) if m == 0 else (lane >= width // 2)
                q[2 * h + m] = jnp.where(mine, scaled_q, 0.0).astype(BF16)
            kv[0, h] = dot(take, k_in[...]).astype(BF16)
            kv[1, h] = dot(take, v_in[...]).astype(BF16)

    def pick_tables():
        lane_slot = lax.broadcasted_iota(jnp.int32, (rows, slots), 1).astype(F32)
        for p in range(picks):
            pick[p] = (lane_slot == as_column(slot_row[p])).astype(F32).astype(BF16)
            pick_w[p] = jnp.transpose(jnp.broadcast_to(route_w_t[p:p + 1, :], (128, rows)))

    length = items
    value_width = kv.shape[3]
    ones = jnp.ones((length, LANES), BF16)

    def across(column, lanes):
        return jnp.concatenate([column] * (lanes // LANES), axis=1)

    def attend(keys_values, diagonal):
        for h in range(heads):
            key = keys_values[0, h]
            value = jnp.concatenate([keys_values[1, h], ones], axis=1)
            for m in range(2):
                n = 2 * h + m
                scores = dot_t(q[n], key)
                if diagonal:
                    q_pos = lax.broadcasted_iota(jnp.int32, scores.shape, 0)
                    k_pos = lax.broadcasted_iota(jnp.int32, scores.shape, 1)
                    scores = jnp.where(k_pos <= q_pos, scores, NEG_FILL)
                high = jnp.max(scores, axis=1, keepdims=True)
                if diagonal:
                    high = jnp.broadcast_to(high, (length, LANES))
                else:
                    old = top[n]
                    high = jnp.maximum(high, old)
                    shrink = jnp.exp(old - high)
                w = jnp.exp(scores - across(high, length)).astype(BF16)
                both = dot(w, value)
                v, s = both[:, :value_width], both[:, value_width:]
                top[n] = high
                norm_sum[n] = s if diagonal else norm_sum[n] * shrink + s
                weighted[n] = v if diagonal else weighted[n] * across(shrink, value_width) + v

    relay = n_ep == 4

    def kv_copy(d):
        return send(kv, kv_all.at[e], kv_s.at[d - 1], kv_r.at[e], ((e + d) % n_ep, t))

    def kv_got(origin):
        return send(kv, kv_all.at[origin], kv_s.at[0], kv_r.at[origin], (origin, t))

    def kv_half(origin, half, device, own=False):
        place = kv_all.at[origin, half]
        return send(kv.at[half] if own else place, place, kh_s.at[origin, half],
                    kh_r.at[origin, half], (device, t))

    def kv_early(action):
        if relay:
            @pl.when(e % 2 == 0)
            def _():
                action(kv_copy(1))

            @pl.when(e == 1)
            def _():
                action(kv_copy(2))
        else:
            loop(1, n_ep - e, lambda d: action(kv_copy(d)))

    def kv_middle(action):
        if relay:
            @pl.when(e == 0)
            def _():
                action(kv_half(0, 1, 2, True))

    def kv_late(action):
        if relay:
            @pl.when(e == 0)
            def _():
                action(kv_half(0, 0, 2, True))

    def kv_second(action):
        if relay:
            @pl.when(e == 2)
            def _():
                action(kv_half(0, 1, 3))

    def kv_pass(origin, action):
        if relay:
            @pl.when((e == 1) & (origin == 0))
            def _():
                action(kv_half(0, 0, 3))

            @pl.when((e == 3) & (origin == 1))
            def _():
                for half in range(2):
                    action(kv_half(1, half, 2))

    def far_origin(j):
        if relay:
            return jnp.where(e == 3, (j + 1) % 3, j)
        return e - 1 - j

    def attend_far(lower, upper):
        def body(j):
            origin = far_origin(j)
            if relay:
                halves = (e == 2) | ((e == 3) & (origin == 0))

                @pl.when(halves)
                def _():
                    kv_half(origin, 0, 3).wait_recv()

                @pl.when(halves & ((e == 3) | (origin == 1)))
                def _():
                    kv_half(origin, 1, 3).wait_recv()

                @pl.when(jnp.logical_not(halves))
                def _():
                    kv_got(origin).wait_recv()
            else:
                kv_got(origin).wait_recv()
            kv_pass(origin, lambda copy: copy.start())
            attend(kv_all.at[origin], False)

        loop(lower, jnp.minimum(upper, e), body)

    with jax.named_scope("dispatch_own"):
        dispatch(z, tok[...])
    with jax.named_scope("unpack"):
        unpack()
    for r in range(nz - 1):
        got_up = has_dn & (z - 1 - r >= 0)
        got_dn = has_up & (z + 1 + r < nz)

        with jax.named_scope("shard_wait"):
            @pl.when(got_up)
            def _():
                shard_copy(0, r, z - 1 - r).wait_recv()

            @pl.when(got_dn)
            def _():
                shard_copy(1, r, z + 1 + r).wait_recv()

            if r < nz - 2:
                shard_sends(r + 1)

        with jax.named_scope("dispatch"):
            @pl.when(got_up)
            def _():
                dispatch(z - 1 - r, held[z - 1 - r])

            @pl.when(got_dn)
            def _():
                dispatch(z + 1 + r, held[z + 1 + r])

        if r == 0:
            with jax.named_scope("diag"):
                attend(kv, True)
                pick_tables()

    kv_early(lambda copy: copy.start())

    def pass_on(k):
        def body(d):
            incoming(k, d).wait_recv()
            forward(k, d).start()

        loop(1, n_ep, body)

    for copy in weights:
        copy.wait()
    gate_sum[...] = jnp.zeros_like(gate_sum)
    up_sum[...] = jnp.zeros_like(up_sum)
    squares[...] = jnp.zeros_like(squares)
    width_total = gain.shape[2] * n_tp
    deep = CORES * shard

    def absorb(k):
        loop(0, n_ep, lambda d: forwarded(k, d).wait_recv())

        def prepare(source):
            place = pl.ds(pl.multiple_of(source * pad, pad), pad)
            for x in range(local):
                for half in range(CORES):
                    floats = arrived[CORES * k + half, source, x * pad:(x + 1) * pad, :].astype(F32)
                    squares[x, place, :] += floats * floats
                    normed[x, place, half * shard:(half + 1) * shard] = (
                        floats * gain[CORES * k + half]).astype(BF16)

        loop(0, n_ep, prepare)
        depth = pl.ds(pl.multiple_of(k * deep, deep), deep)
        for x in range(local):
            gate_sum[x] += dot(normed[x], gate[x, depth, :])
            up_sum[x] += dot(normed[x], up[x, depth, :])

    def visit(i, action):
        k = z - (i + 1) // 2 * (i % 2) + i // 2 * (1 - i % 2)

        @pl.when((k >= 0) & (k < nz))
        def _():
            action(k)

    def arrival(i):
        @pl.when(i < 2 * nz - 1)
        def _():
            visit(i, pass_on)

        @pl.when(i == 2 * nz - 2)
        def _():
            kv_middle(lambda copy: copy.start())

        @pl.when(i >= 2)
        def _():
            visit(i - 2, absorb)

    with jax.named_scope("absorb"):
        loop(0, 2 * nz + 1, arrival)

    count = n_ep * pad

    def goal(i):
        down, up_to = nz - 1 - i, i
        down = jnp.where(down <= z, down - 1, down)
        up_to = jnp.where(up_to >= z, up_to + 1, up_to)
        return jnp.where(i == nz - 1, z, jnp.where(2 * z < nz, down, up_to))

    def pair_copy(k):
        return send(part.at[1 - c, k], pair.at[k], pr_s.at[k], pr_r.at[k], (e, partner))

    def exchange(k, d):
        target = (e + d) % n_ep
        return send(fin.at[k, target], ex.at[k, e], ex_s.at[k, d - 1], ex_r.at[k, d - 1], (target, t))

    def exchanged(k, d):
        origin = (e + n_ep - d) % n_ep
        return send(fin.at[k, origin], ex.at[k, origin], ex_s.at[k, d - 1], ex_r.at[k, d - 1],
                    (origin, t))

    def slot_copy(way):
        k = z + 1 if way == 0 else z - 1
        target = t + CORES if way == 0 else t - CORES
        return send(fin.at[k], slot_got.at[way], sl_s.at[way], sl_r.at[way], (e, target))

    def slot_recv(way):
        return send(fin.at[z], slot_got.at[way], sl_s.at[way], sl_r.at[way], (e, partner))

    def token_copy(k):
        return send(tok_stage.at[k], tok_got.at[z], tk_s.at[k], tk_r.at[z], (e, CORES * k + c))

    def token_got(k):
        return send(tok_stage.at[k], tok_got.at[k], tk_s.at[k], tk_r.at[k], (e, CORES * k + c))

    def is_far(k):
        return (k > z + 1) | (k < z - 1)

    with jax.named_scope("hidden"):
        for x in range(local):
            mean = jnp.sum(squares[x], axis=1, keepdims=True) / width_total
            factor = lax.rsqrt(mean + NORM_EPS)
            gate_pre = jnp.minimum(gate_sum[x] * factor, CLAMP_LIMIT)
            up_pre = jnp.clip(up_sum[x] * factor, -CLAMP_LIMIT, CLAMP_LIMIT)
            hidden[x] = ((up_pre + 1.0) * gate_pre * jax.nn.sigmoid(GLU_ALPHA * gate_pre)).astype(BF16)

    def project(i):
        k = goal(i)
        place = pl.ds(pl.multiple_of(k * deep, deep), deep)
        for x in range(local):
            product = dot(hidden[x], down[x, :, place]).astype(BF16)
            for half in range(CORES):
                part[half, k, x] = product[:, half * shard:(half + 1) * shard]
        pair_copy(k).start()

    def finish(i):
        k = goal(i)
        pair_copy(k).wait_recv()
        for x in range(local):
            both = (part[c, k, x].astype(F32) + pair[k, x].astype(F32)).astype(BF16)
            for source in range(n_ep):
                fin[k, source, x * pad:(x + 1) * pad, :] = both[source * pad:(source + 1) * pad, :]

        @pl.when(is_far(k))
        def _():
            loop(1, n_ep, lambda d: exchange(k, d).start())

        @pl.when(k == z + 1)
        def _():
            slot_copy(0).start()

        @pl.when(k == z - 1)
        def _():
            slot_copy(1).start()

    def step(i):
        @pl.when(i < nz)
        def _():
            project(i)

        @pl.when(i >= 2)
        def _():
            finish(i - 2)

    with jax.named_scope("finish"):
        loop(0, nz + 2, step)
        kv_late(lambda copy: copy.start())

    def mixture(results):
        mixed = None
        for p in range(picks):
            selected = dot(pick[p], results)
            weight = jnp.concatenate([pick_w[p]] * (shard // 128), axis=1)
            mixed = selected * weight if mixed is None else mixed + selected * weight
        return mixed

    def tokens_out(i):
        k = goal(i)

        @pl.when(is_far(k))
        def _():
            ex[k, e] = fin[k, e]
            loop(1, n_ep, lambda d: exchanged(k, d).wait_recv())
            tok_stage[k] = mixture(ex[k].reshape(slots, shard)).astype(BF16)
            token_copy(k).start()

    early = jnp.where(e == 2, 0, e) if relay else 0
    early = jnp.minimum(early, 2)
    with jax.named_scope("second"):
        if relay:
            @pl.when(e == 2)
            def _():
                kv_half(0, 1, 3).wait_recv()
                kv_half(0, 1, 3).start()
    with jax.named_scope("far0"):
        attend_far(0, early)
    with jax.named_scope("tokens_out"):
        loop(0, nz, tokens_out)
    with jax.named_scope("slots_in"):
        @pl.when(has_dn)
        def _():
            slot_recv(0).wait_recv()

        @pl.when(has_up)
        def _():
            slot_recv(1).wait_recv()

        for x in range(local):
            span = slice(x * pad, (x + 1) * pad)
            for source in range(n_ep):
                total = fin[z, source, span, :].astype(F32)
                low = slot_got[0, source, span, :].astype(F32)
                high = slot_got[1, source, span, :].astype(F32)
                total = total + jnp.where(has_dn, low, 0.0) + jnp.where(has_up, high, 0.0)
                final[source, span, :] = total.astype(BF16)

    def give(d):
        return send(final.at[(e + d) % n_ep], back.at[e], rt_s.at[d - 1], rt_r.at[d - 1],
                    ((e + d) % n_ep, t))

    def given(d):
        origin = (e + n_ep - d) % n_ep
        return send(final.at[origin], back.at[origin], rt_s.at[d - 1], rt_r.at[d - 1], (origin, t))

    loop(1, n_ep, lambda d: give(d).start())
    back[e] = final[e]

    with jax.named_scope("far2"):
        attend_far(early, n_ep)
    with jax.named_scope("attn_fin"):
        for h in range(heads):
            first, second = (
                weighted[n] / across(norm_sum[n], value_width) for n in (2 * h, 2 * h + 1))
            blend = first - mix[h] * second
            mean = jnp.mean(blend * blend, axis=1, keepdims=True)
            scaled = (blend * lax.rsqrt(mean + SUB_EPS) * sub_gain[...] * OUT_SCALE).astype(BF16)
            put_i = lax.broadcasted_iota(jnp.int32, (items * heads, items), 0)
            of_i = lax.broadcasted_iota(jnp.int32, (items * heads, items), 1)
            placed = dot((put_i == of_i * heads + h).astype(F32).astype(BF16), scaled)
            woven = placed if h == 0 else woven + placed
        attn_out[...] = woven.astype(BF16)

    with jax.named_scope("send_waits"):
        for r in range(nz - 1):
            shard_send_waits(r)
        loop(0, nz, lambda k: loop(1, n_ep, lambda d: piece(k, d).wait_send()))
        loop(0, nz, lambda k: loop(0, n_ep, lambda d: forward(k, d).wait_send()))
        loop(0, nz, lambda k: pair_copy(k).wait_send())

        def far_waits(k):
            @pl.when(is_far(k))
            def _():
                loop(1, n_ep, lambda d: exchange(k, d).wait_send())
                token_copy(k).wait_send()

        loop(0, nz, far_waits)

        @pl.when(has_up)
        def _():
            slot_copy(0).wait_send()

        @pl.when(has_dn)
        def _():
            slot_copy(1).wait_send()

    with jax.named_scope("tokens_in"):
        held_sum[...] = jnp.zeros_like(held_sum)

        def add_far(k):
            @pl.when(is_far(k))
            def _():
                token_got(k).wait_recv()
                held_sum[...] += tok_got[k].astype(F32)

        loop(0, nz, add_far)

    with jax.named_scope("given_wait"):
        loop(1, n_ep, lambda d: given(d).wait_recv())
    with jax.named_scope("combine"):
        moe_out[...] = (mixture(back[...].reshape(slots, shard)) + held_sum[...]).astype(BF16)
        loop(1, n_ep, lambda d: give(d).wait_send())
        for part_of in (kv_early, kv_middle, kv_late, kv_second):
            part_of(lambda copy: copy.wait_send())
        if relay:
            for origin in range(2):
                kv_pass(origin, lambda copy: copy.wait_send())


def make_shards(n_ep, n_tp):
    def shards(
        queries, keys, values, mix_weight, sub_gain, tokens, routes, route_weights,
        expert_gain, gate_weight, up_weight, down_weight,
    ):
        rows, shard = tokens.shape
        picks = routes.shape[1]
        local, depth, units = gate_weight.shape
        cap = 3 * rows * picks // (2 * n_ep * local)
        pad = -(-cap // 16) * 16
        length, heads, width = queries.shape
        value_width = values.shape[2]
        nz = n_tp // CORES
        block = local * pad
        count = n_ep * pad
        vmem = pl.BlockSpec(memory_space=pltpu.VMEM)
        hbm = pl.BlockSpec(memory_space=pltpu.HBM)
        dma = pltpu.SemaphoreType.DMA
        peers = n_ep - 1
        attn, moe = pl.pallas_call(
            functools.partial(layer_kernel, n_ep, n_tp, cap, heads, pad),
            out_shape=(
                pltpu.VMEM((length * heads, value_width), BF16),
                pltpu.VMEM((rows, shard), BF16),
            ),
            in_specs=[hbm] * 11 + [pl.BlockSpec(memory_space=pltpu.SMEM)],
            out_specs=(vmem, vmem),
            scratch_shapes=[
                pltpu.VMEM((rows, shard), BF16),
                pltpu.VMEM((picks, rows), jnp.int32),
                pltpu.VMEM((picks, rows), F32),
                pltpu.VMEM((n_tp, 1, shard), F32),
                pltpu.VMEM((length * heads, width), BF16),
                pltpu.VMEM((length * heads, width), BF16),
                pltpu.VMEM((length * heads, value_width), BF16),
                pltpu.VMEM((1, value_width), F32),
                pltpu.VMEM(gate_weight.shape, BF16),
                pltpu.VMEM(up_weight.shape, BF16),
                pltpu.VMEM(down_weight.shape, BF16),
                pltpu.VMEM((nz, rows, shard), BF16),
                pltpu.VMEM((nz, n_ep, block, shard), BF16),
                pltpu.VMEM((n_tp, n_ep, block, shard), BF16),
                pltpu.VMEM((local, count, CORES * shard), BF16),
                pltpu.VMEM((local, count, shard), F32),
                pltpu.VMEM((local, count, units), F32),
                pltpu.VMEM((local, count, units), F32),
                pltpu.VMEM((local, count, units), BF16),
                pltpu.VMEM((CORES, nz, local, count, shard), BF16),
                pltpu.VMEM((nz, local, count, shard), BF16),
                pltpu.VMEM((nz, n_ep, block, shard), BF16),
                pltpu.VMEM((nz, n_ep, block, shard), BF16),
                pltpu.VMEM((2, n_ep, block, shard), BF16),
                pltpu.VMEM((nz, rows, shard), BF16),
                pltpu.VMEM((nz, rows, shard), BF16),
                pltpu.VMEM((rows, shard), F32),
                pltpu.VMEM((n_ep, block, shard), BF16),
                pltpu.VMEM((n_ep, block, shard), BF16),
                pltpu.VMEM((picks, rows, n_ep * block), BF16),
                pltpu.VMEM((picks, rows, 128), F32),
                pltpu.VMEM((2 * heads, length, width), BF16),
                pltpu.VMEM((2, heads, length, width), BF16),
                pltpu.VMEM((n_ep, 2, heads, length, width), BF16),
                pltpu.VMEM((2 * heads, length, LANES), F32),
                pltpu.VMEM((2 * heads, length, LANES), F32),
                pltpu.VMEM((2 * heads, length, value_width), F32),
                dma((8,)),
                dma((3,)),
                dma((2, nz - 1)), dma((2, nz - 1)),
                dma((nz, peers)), dma((nz, peers)),
                dma((nz, n_ep)), dma((nz, n_ep)),
                dma((max(peers, 2),)), dma((n_ep,)),
                dma((2, 2)), dma((2, 2)),
                dma((nz,)), dma((nz,)),
                dma((nz, peers)), dma((nz, peers)),
                dma((2,)), dma((2,)),
                dma((nz,)), dma((nz,)),
                dma((peers,)), dma((peers,)),
            ],
            compiler_params=pltpu.CompilerParams(
                collective_id=0, has_side_effects=True, vmem_limit_bytes=54 * 2**20),
            name="layer",
        )(*(pltpu.with_memory_space_constraint(x, pltpu.HBM) for x in (
            tokens, jnp.transpose(routes), jnp.transpose(route_weights),
            expert_gain.reshape(n_tp, 1, shard), gate_weight, up_weight, down_weight,
            queries.reshape(length * heads, width), keys.reshape(length * heads, width),
            values.reshape(length * heads, value_width), sub_gain[None, :],
        )), mix_weight)
        return attn.reshape(length, heads, value_width), moe

    return shards


def solution(mesh):
    return jax.shard_map(
        make_shards(mesh.shape["ep"], mesh.shape["tp"]),
        mesh=mesh,
        in_specs=(
            P("ep", "tp", None),
            P("ep", "tp", None),
            P("ep", "tp", None),
            P("tp"),
            P(),
            P("ep", "tp"),
            P("ep", None),
            P("ep", None),
            P(),
            P("ep", None, "tp"),
            P("ep", None, "tp"),
            P("ep", "tp", None),
        ),
        out_specs=(P("ep", "tp", None), P("ep", "tp")),
        check_vma=False,
    )
```

```python
import functools

import jax
import jax.numpy as jnp
from jax import lax
from jax.experimental import pallas as pl
from jax.experimental.pallas import tpu as pltpu
from jax.sharding import PartitionSpec as P

NEG_FILL = -1e30
SUB_EPS = 1e-05
NORM_EPS = 1e-06
CLAMP_LIMIT = 7.0
GLU_ALPHA = 1.702
OUT_SCALE = 0.8
CORES = 2
LANES = 128
F32 = jnp.float32
BF16 = jnp.bfloat16
MESH = pl.DeviceIdType.MESH


def dot(a, b):
    return jnp.dot(a, b, preferred_element_type=F32)


def dot_t(a, b):
    return lax.dot_general(a, b, (((1,), (1,)), ((), ())), preferred_element_type=F32)


def loop(lower, upper, body):
    def step(index, carry):
        body(index)
        return carry

    lax.fori_loop(lower, upper, step, 0)


def layer_kernel(
    n_ep, n_tp, cap, heads, rank_pad,
    tok_hbm, routes_hbm, route_w_hbm, gain_hbm, gate_hbm, up_hbm, down_hbm,
    q_hbm, k_hbm, v_hbm, sub_gain_hbm, mix,
    attn_out, moe_out,
    tok, routes_t, route_w_t, gain, q_in, k_in, v_in, sub_gain,
    gate, up, down, held, outgoing, arrived, normed, squares, gate_sum, up_sum, hidden, part, pair,
    fin, ex, slot_got, tok_stage, tok_got, held_sum, final, back, pick, pick_w, q, kv, kv_all,
    top, norm_sum, weighted,
    in_sem, w_sem, ag_s, ag_r, dp_s, dp_r, fw_s, fw_r, kv_s, kv_r, kh_s, kh_r, kq_s, kq_r, pr_s, pr_r,
    ex_s, ex_r, sl_s, sl_r, tk_s, tk_r, rt_s, rt_r,
):
    e, t = lax.axis_index("ep"), lax.axis_index("tp")
    nz = n_tp // CORES
    z, c = t // CORES, t % CORES
    partner = t + 1 - 2 * c
    rows, shard = tok.shape
    local = gate_hbm.shape[0]
    experts = n_ep * local
    pad = rank_pad
    slots = experts * pad
    block = local * pad
    has_up, has_dn = z < nz - 1, z > 0

    loads = [
        pltpu.make_async_copy(source, target, in_sem.at[i])
        for i, (source, target) in enumerate((
            (tok_hbm, tok), (routes_hbm, routes_t), (route_w_hbm, route_w_t), (gain_hbm, gain),
            (q_hbm, q_in), (k_hbm, k_in), (v_hbm, v_in), (sub_gain_hbm, sub_gain)))
    ]
    for copy in loads:
        copy.start()
    weights = [
        pltpu.make_async_copy(source, target, w_sem.at[i])
        for i, (source, target) in enumerate(((gate_hbm, gate), (up_hbm, up), (down_hbm, down)))
    ]
    for copy in weights:
        copy.start()

    barrier = pltpu.get_barrier_semaphore()
    pl.semaphore_signal(barrier, inc=1, device_id=(e, partner), device_id_type=MESH)

    @pl.when(has_up)
    def _():
        pl.semaphore_signal(barrier, inc=1, device_id=(e, t + CORES), device_id_type=MESH)

    @pl.when(has_dn)
    def _():
        pl.semaphore_signal(barrier, inc=1, device_id=(e, t - CORES), device_id_type=MESH)

    loop(1, n_ep, lambda d: pl.semaphore_signal(
        barrier, inc=1, device_id=((e + d) % n_ep, t), device_id_type=MESH))
    for copy in loads[:2]:
        copy.wait()
    with jax.named_scope("barrier"):
        pl.semaphore_wait(barrier, n_ep + has_up.astype(jnp.int32) + has_dn.astype(jnp.int32))

    def send(source, target, s_sem, r_sem, device):
        return pltpu.make_async_remote_copy(
            src_ref=source, dst_ref=target, send_sem=s_sem, recv_sem=r_sem,
            device_id=device, device_id_type=MESH)

    def shard_copy(way, r, origin):
        source = tok if r == 0 else held.at[origin]
        target = t + CORES if way == 0 else t - CORES
        return send(source, held.at[origin], ag_s.at[way, r], ag_r.at[way, r], (e, target))

    def shard_sends(r):
        @pl.when(has_up & (z - r >= 0))
        def _():
            shard_copy(0, r, z - r).start()

        @pl.when(has_dn & (z + r < nz))
        def _():
            shard_copy(1, r, z + r).start()

    def shard_send_waits(r):
        @pl.when(has_up & (z - r >= 0))
        def _():
            shard_copy(0, r, z - r).wait_send()

        @pl.when(has_dn & (z + r < nz))
        def _():
            shard_copy(1, r, z + r).wait_send()

    shard_sends(0)

    row_i = lax.broadcasted_iota(jnp.int32, (rows, rows), 0)
    col_i = lax.broadcasted_iota(jnp.int32, (rows, rows), 1)
    picks = routes_t.shape[0]
    exp_row = lax.broadcasted_iota(jnp.int32, (experts, rows), 0)
    hot_t = [(routes_t[p:p + 1, :] == exp_row).astype(F32) for p in range(picks)]
    before_t = dot(sum(hot_t).astype(BF16), (row_i < col_i).astype(F32).astype(BF16))
    slot_row = [
        jnp.sum(h * (before_t + (exp_row * pad).astype(F32)), axis=0, keepdims=True)
        for h in hot_t
    ]
    slot_i = lax.broadcasted_iota(jnp.int32, (slots, rows), 0).astype(F32)

    def as_column(line):
        return jnp.transpose(jnp.broadcast_to(line, (128, rows)))[:, :1]

    choose = sum((slot_i == s).astype(F32) for s in slot_row).astype(BF16)

    def piece(k, d):
        source = outgoing.at[k, (e + d) % n_ep]
        return send(source, arrived.at[CORES * k + c, e], dp_s.at[k, d - 1], dp_r.at[k, d - 1],
                    ((e + d) % n_ep, t))

    def incoming(k, d):
        origin = (e + n_ep - d) % n_ep
        return send(outgoing.at[k, origin], arrived.at[CORES * k + c, origin],
                    dp_s.at[k, d - 1], dp_r.at[k, d - 1], (origin, t))

    def forward(k, d):
        origin = (e + n_ep - d) % n_ep
        place = arrived.at[CORES * k + c, origin]
        return send(place, place, fw_s.at[k, d], fw_r.at[k, d], (e, partner))

    def forwarded(k, d):
        origin = (e + n_ep - d) % n_ep
        place = arrived.at[CORES * k + 1 - c, origin]
        return send(place, place, fw_s.at[k, d], fw_r.at[k, d], (e, partner))

    def dispatch(k, source):
        made = dot(choose, source).astype(BF16).reshape(n_ep, block, shard)
        outgoing[k] = made
        arrived[CORES * k + c, e] = outgoing[k, e]
        loop(1, n_ep, lambda d: piece(k, d).start())
        forward(k, 0).start()

    items, width = q.shape[1:]

    def unpack():
        for copy in loads[2:]:
            copy.wait()
        pick_i = lax.broadcasted_iota(jnp.int32, (items, items * heads), 0)
        from_i = lax.broadcasted_iota(jnp.int32, (items, items * heads), 1)
        for h in range(heads):
            take = (from_i == pick_i * heads + h).astype(F32).astype(BF16)
            scaled_q = dot(take, q_in[...]) * (width // 2) ** -0.5
            lane = lax.broadcasted_iota(jnp.int32, (items, width), 1)
            for m in range(2):
                mine = (lane < width // 2) if m == 0 else (lane >= width // 2)
                q[2 * h + m] = jnp.where(mine, scaled_q, 0.0).astype(BF16)
            kv[0, h] = dot(take, k_in[...]).astype(BF16)
            kv[1, h] = dot(take, v_in[...]).astype(BF16)

    def pick_tables():
        lane_slot = lax.broadcasted_iota(jnp.int32, (rows, slots), 1).astype(F32)
        for p in range(picks):
            pick[p] = (lane_slot == as_column(slot_row[p])).astype(F32).astype(BF16)
            pick_w[p] = jnp.transpose(jnp.broadcast_to(route_w_t[p:p + 1, :], (128, rows)))

    length = items
    value_width = kv.shape[3]
    ones = jnp.ones((length, LANES), BF16)

    def across(column, lanes):
        return jnp.concatenate([column] * (lanes // LANES), axis=1)

    def attend(keys_values, diagonal):
        for h in range(heads):
            key = keys_values[0, h]
            value = jnp.concatenate([keys_values[1, h], ones], axis=1)
            for m in range(2):
                n = 2 * h + m
                scores = dot_t(q[n], key)
                if diagonal:
                    q_pos = lax.broadcasted_iota(jnp.int32, scores.shape, 0)
                    k_pos = lax.broadcasted_iota(jnp.int32, scores.shape, 1)
                    scores = jnp.where(k_pos <= q_pos, scores, NEG_FILL)
                high = jnp.max(scores, axis=1, keepdims=True)
                if diagonal:
                    high = jnp.broadcast_to(high, (length, LANES))
                else:
                    old = top[n]
                    high = jnp.maximum(high, old)
                    shrink = jnp.exp(old - high)
                w = jnp.exp(scores - across(high, length)).astype(BF16)
                both = dot(w, value)
                v, s = both[:, :value_width], both[:, value_width:]
                top[n] = high
                norm_sum[n] = s if diagonal else norm_sum[n] * shrink + s
                weighted[n] = v if diagonal else weighted[n] * across(shrink, value_width) + v

    relay = n_ep == 4

    def kv_copy(d):
        return send(kv, kv_all.at[e], kv_s.at[d - 1], kv_r.at[e], ((e + d) % n_ep, t))

    def kv_got(origin):
        return send(kv, kv_all.at[origin], kv_s.at[0], kv_r.at[origin], (origin, t))

    def kv_half(origin, half, device, own=False):
        place = kv_all.at[origin, half]
        return send(kv.at[half] if own else place, place, kh_s.at[origin, half],
                    kh_r.at[origin, half], (device, t))

    def kv_early(action):
        if relay:
            @pl.when(e % 2 == 0)
            def _():
                action(kv_copy(1))

            @pl.when(e == 1)
            def _():
                action(kv_copy(2))
        else:
            loop(1, n_ep - e, lambda d: action(kv_copy(d)))

    def kv_middle(action):
        if relay:
            @pl.when(e == 0)
            def _():
                action(kv_half(0, 1, 2, True))

    def kv_late(action):
        if relay:
            @pl.when(e == 0)
            def _():
                action(kv_half(0, 0, 2, True))

            if near:
                @pl.when(e == 1)
                def _():
                    action(kv_heads(True))

    def kv_second(action):
        if relay:
            @pl.when(e == 2)
            def _():
                action(kv_half(0, 1, 3))

    near = heads // 2

    def kv_heads(own):
        span = pl.ds(0, near) if own else pl.ds(near, heads - near)
        place = kv_all.at[1, 1, span]
        index = 0 if own else 1
        return send(kv.at[1, span] if own else place, place, kq_s.at[index], kq_r.at[index], (2, t))

    def kv_pass(origin, action):
        if relay:
            @pl.when((e == 1) & (origin == 0))
            def _():
                action(kv_half(0, 0, 3))

            @pl.when((e == 3) & (origin == 1))
            def _():
                action(kv_half(1, 0, 2))
                action(kv_heads(False))

    def far_origin(j):
        if relay:
            return jnp.where(e == 3, (j + 1) % 3, j)
        return e - 1 - j

    def attend_far(lower, upper):
        def body(j):
            origin = far_origin(j)
            if relay:
                halves = (e == 2) | ((e == 3) & (origin == 0))

                @pl.when(halves)
                def _():
                    kv_half(origin, 0, 3).wait_recv()

                @pl.when(halves & (e == 3))
                def _():
                    kv_half(origin, 1, 3).wait_recv()

                @pl.when(halves & (e == 2) & (origin == 1))
                def _():
                    kv_heads(False).wait_recv()
                    if near:
                        kv_heads(True).wait_recv()

                @pl.when(jnp.logical_not(halves))
                def _():
                    kv_got(origin).wait_recv()
            else:
                kv_got(origin).wait_recv()
            kv_pass(origin, lambda copy: copy.start())
            attend(kv_all.at[origin], False)

        loop(lower, jnp.minimum(upper, e), body)

    with jax.named_scope("dispatch_own"):
        dispatch(z, tok[...])
    with jax.named_scope("unpack"):
        unpack()
    for r in range(nz - 1):
        got_up = has_dn & (z - 1 - r >= 0)
        got_dn = has_up & (z + 1 + r < nz)

        with jax.named_scope("shard_wait"):
            @pl.when(got_up)
            def _():
                shard_copy(0, r, z - 1 - r).wait_recv()

            @pl.when(got_dn)
            def _():
                shard_copy(1, r, z + 1 + r).wait_recv()

            if r < nz - 2:
                shard_sends(r + 1)

        with jax.named_scope("dispatch"):
            @pl.when(got_up)
            def _():
                dispatch(z - 1 - r, held[z - 1 - r])

            @pl.when(got_dn)
            def _():
                dispatch(z + 1 + r, held[z + 1 + r])

        if r == 0:
            with jax.named_scope("diag"):
                attend(kv, True)
                pick_tables()

    kv_early(lambda copy: copy.start())

    def pass_on(k):
        def body(d):
            incoming(k, d).wait_recv()
            forward(k, d).start()

        loop(1, n_ep, body)

    for copy in weights:
        copy.wait()
    gate_sum[...] = jnp.zeros_like(gate_sum)
    up_sum[...] = jnp.zeros_like(up_sum)
    squares[...] = jnp.zeros_like(squares)
    width_total = gain.shape[2] * n_tp
    deep = CORES * shard

    def absorb(k):
        loop(0, n_ep, lambda d: forwarded(k, d).wait_recv())

        def prepare(source):
            place = pl.ds(pl.multiple_of(source * pad, pad), pad)
            for x in range(local):
                for half in range(CORES):
                    floats = arrived[CORES * k + half, source, x * pad:(x + 1) * pad, :].astype(F32)
                    squares[x, place, :] += floats * floats
                    normed[x, place, half * shard:(half + 1) * shard] = (
                        floats * gain[CORES * k + half]).astype(BF16)

        loop(0, n_ep, prepare)
        depth = pl.ds(pl.multiple_of(k * deep, deep), deep)
        for x in range(local):
            gate_sum[x] += dot(normed[x], gate[x, depth, :])
            up_sum[x] += dot(normed[x], up[x, depth, :])

    def visit(i, action):
        k = z - (i + 1) // 2 * (i % 2) + i // 2 * (1 - i % 2)

        @pl.when((k >= 0) & (k < nz))
        def _():
            action(k)

    def arrival(i):
        @pl.when(i < 2 * nz - 1)
        def _():
            visit(i, pass_on)

        @pl.when(i == 2 * nz - 2)
        def _():
            kv_middle(lambda copy: copy.start())

        @pl.when(i >= 2)
        def _():
            visit(i - 2, absorb)

    with jax.named_scope("absorb"):
        loop(0, 2 * nz + 1, arrival)

    count = n_ep * pad

    def goal(i):
        down, up_to = nz - 1 - i, i
        down = jnp.where(down <= z, down - 1, down)
        up_to = jnp.where(up_to >= z, up_to + 1, up_to)
        return jnp.where(i == nz - 1, z, jnp.where(2 * z < nz, down, up_to))

    def pair_copy(k):
        return send(part.at[1 - c, k], pair.at[k], pr_s.at[k], pr_r.at[k], (e, partner))

    def exchange(k, d):
        target = (e + d) % n_ep
        return send(fin.at[k, target], ex.at[k, e], ex_s.at[k, d - 1], ex_r.at[k, d - 1], (target, t))

    def exchanged(k, d):
        origin = (e + n_ep - d) % n_ep
        return send(fin.at[k, origin], ex.at[k, origin], ex_s.at[k, d - 1], ex_r.at[k, d - 1],
                    (origin, t))

    def slot_copy(way):
        k = z + 1 if way == 0 else z - 1
        target = t + CORES if way == 0 else t - CORES
        return send(fin.at[k], slot_got.at[way], sl_s.at[way], sl_r.at[way], (e, target))

    def slot_recv(way):
        return send(fin.at[z], slot_got.at[way], sl_s.at[way], sl_r.at[way], (e, partner))

    def token_copy(k):
        return send(tok_stage.at[k], tok_got.at[z], tk_s.at[k], tk_r.at[z], (e, CORES * k + c))

    def token_got(k):
        return send(tok_stage.at[k], tok_got.at[k], tk_s.at[k], tk_r.at[k], (e, CORES * k + c))

    def is_far(k):
        return (k > z + 1) | (k < z - 1)

    with jax.named_scope("hidden"):
        for x in range(local):
            mean = jnp.sum(squares[x], axis=1, keepdims=True) / width_total
            factor = lax.rsqrt(mean + NORM_EPS)
            gate_pre = jnp.minimum(gate_sum[x] * factor, CLAMP_LIMIT)
            up_pre = jnp.clip(up_sum[x] * factor, -CLAMP_LIMIT, CLAMP_LIMIT)
            hidden[x] = ((up_pre + 1.0) * gate_pre * jax.nn.sigmoid(GLU_ALPHA * gate_pre)).astype(BF16)

    def project(i):
        k = goal(i)
        place = pl.ds(pl.multiple_of(k * deep, deep), deep)
        for x in range(local):
            product = dot(hidden[x], down[x, :, place]).astype(BF16)
            for half in range(CORES):
                part[half, k, x] = product[:, half * shard:(half + 1) * shard]
        pair_copy(k).start()

    def finish(i):
        k = goal(i)
        pair_copy(k).wait_recv()
        for x in range(local):
            both = (part[c, k, x].astype(F32) + pair[k, x].astype(F32)).astype(BF16)
            for source in range(n_ep):
                fin[k, source, x * pad:(x + 1) * pad, :] = both[source * pad:(source + 1) * pad, :]

        @pl.when(is_far(k))
        def _():
            loop(1, n_ep, lambda d: exchange(k, d).start())

        @pl.when(k == z + 1)
        def _():
            slot_copy(0).start()

        @pl.when(k == z - 1)
        def _():
            slot_copy(1).start()

    def step(i):
        @pl.when(i < nz)
        def _():
            project(i)

        @pl.when(i >= 2)
        def _():
            finish(i - 2)

    with jax.named_scope("finish"):
        loop(0, nz + 2, step)
        kv_late(lambda copy: copy.start())

    def mixture(results):
        mixed = None
        for p in range(picks):
            selected = dot(pick[p], results)
            weight = jnp.concatenate([pick_w[p]] * (shard // 128), axis=1)
            mixed = selected * weight if mixed is None else mixed + selected * weight
        return mixed

    def tokens_out(i):
        k = goal(i)

        @pl.when(is_far(k))
        def _():
            ex[k, e] = fin[k, e]
            loop(1, n_ep, lambda d: exchanged(k, d).wait_recv())
            tok_stage[k] = mixture(ex[k].reshape(slots, shard)).astype(BF16)
            token_copy(k).start()

    early = jnp.where(e == 2, 0, e) if relay else 0
    early = jnp.minimum(early, 2)
    with jax.named_scope("second"):
        if relay:
            @pl.when(e == 2)
            def _():
                kv_half(0, 1, 3).wait_recv()
                kv_half(0, 1, 3).start()
    with jax.named_scope("far0"):
        attend_far(0, early)
    with jax.named_scope("tokens_out"):
        loop(0, nz, tokens_out)
    with jax.named_scope("slots_in"):
        @pl.when(has_dn)
        def _():
            slot_recv(0).wait_recv()

        @pl.when(has_up)
        def _():
            slot_recv(1).wait_recv()

        for x in range(local):
            span = slice(x * pad, (x + 1) * pad)
            for source in range(n_ep):
                total = fin[z, source, span, :].astype(F32)
                low = slot_got[0, source, span, :].astype(F32)
                high = slot_got[1, source, span, :].astype(F32)
                total = total + jnp.where(has_dn, low, 0.0) + jnp.where(has_up, high, 0.0)
                final[source, span, :] = total.astype(BF16)

    def give(d):
        return send(final.at[(e + d) % n_ep], back.at[e], rt_s.at[d - 1], rt_r.at[d - 1],
                    ((e + d) % n_ep, t))

    def given(d):
        origin = (e + n_ep - d) % n_ep
        return send(final.at[origin], back.at[origin], rt_s.at[d - 1], rt_r.at[d - 1], (origin, t))

    loop(1, n_ep, lambda d: give(d).start())
    back[e] = final[e]

    with jax.named_scope("far2"):
        attend_far(early, n_ep)
    with jax.named_scope("attn_fin"):
        for h in range(heads):
            first, second = (
                weighted[n] / across(norm_sum[n], value_width) for n in (2 * h, 2 * h + 1))
            blend = first - mix[h] * second
            mean = jnp.mean(blend * blend, axis=1, keepdims=True)
            scaled = (blend * lax.rsqrt(mean + SUB_EPS) * sub_gain[...] * OUT_SCALE).astype(BF16)
            put_i = lax.broadcasted_iota(jnp.int32, (items * heads, items), 0)
            of_i = lax.broadcasted_iota(jnp.int32, (items * heads, items), 1)
            placed = dot((put_i == of_i * heads + h).astype(F32).astype(BF16), scaled)
            woven = placed if h == 0 else woven + placed
        attn_out[...] = woven.astype(BF16)

    with jax.named_scope("send_waits"):
        for r in range(nz - 1):
            shard_send_waits(r)
        loop(0, nz, lambda k: loop(1, n_ep, lambda d: piece(k, d).wait_send()))
        loop(0, nz, lambda k: loop(0, n_ep, lambda d: forward(k, d).wait_send()))
        loop(0, nz, lambda k: pair_copy(k).wait_send())

        def far_waits(k):
            @pl.when(is_far(k))
            def _():
                loop(1, n_ep, lambda d: exchange(k, d).wait_send())
                token_copy(k).wait_send()

        loop(0, nz, far_waits)

        @pl.when(has_up)
        def _():
            slot_copy(0).wait_send()

        @pl.when(has_dn)
        def _():
            slot_copy(1).wait_send()

    with jax.named_scope("tokens_in"):
        held_sum[...] = jnp.zeros_like(held_sum)

        def add_far(k):
            @pl.when(is_far(k))
            def _():
                token_got(k).wait_recv()
                held_sum[...] += tok_got[k].astype(F32)

        loop(0, nz, add_far)

    with jax.named_scope("given_wait"):
        loop(1, n_ep, lambda d: given(d).wait_recv())
    with jax.named_scope("combine"):
        moe_out[...] = (mixture(back[...].reshape(slots, shard)) + held_sum[...]).astype(BF16)
        loop(1, n_ep, lambda d: give(d).wait_send())
        for part_of in (kv_early, kv_middle, kv_late, kv_second):
            part_of(lambda copy: copy.wait_send())
        if relay:
            for origin in range(2):
                kv_pass(origin, lambda copy: copy.wait_send())


def store_kernel(attn, moe, attn_hbm, moe_hbm, sems):
    copies = [
        pltpu.make_async_copy(source, target, sems.at[i])
        for i, (source, target) in enumerate(((attn, attn_hbm), (moe, moe_hbm)))
    ]
    for copy in copies:
        copy.start()
    for copy in copies:
        copy.wait()


def make_shards(n_ep, n_tp):
    def shards(
        queries, keys, values, mix_weight, sub_gain, tokens, routes, route_weights,
        expert_gain, gate_weight, up_weight, down_weight,
    ):
        rows, shard = tokens.shape
        picks = routes.shape[1]
        local, depth, units = gate_weight.shape
        cap = 3 * rows * picks // (2 * n_ep * local)
        pad = -(-cap // 16) * 16
        length, heads, width = queries.shape
        value_width = values.shape[2]
        nz = n_tp // CORES
        block = local * pad
        count = n_ep * pad
        vmem = pl.BlockSpec(memory_space=pltpu.VMEM)
        hbm = pl.BlockSpec(memory_space=pltpu.HBM)
        dma = pltpu.SemaphoreType.DMA
        peers = n_ep - 1
        attn, moe = pl.pallas_call(
            functools.partial(layer_kernel, n_ep, n_tp, cap, heads, pad),
            out_shape=(
                pltpu.VMEM((length * heads, value_width), BF16),
                pltpu.VMEM((rows, shard), BF16),
            ),
            in_specs=[hbm] * 11 + [pl.BlockSpec(memory_space=pltpu.SMEM)],
            out_specs=(vmem, vmem),
            scratch_shapes=[
                pltpu.VMEM((rows, shard), BF16),
                pltpu.VMEM((picks, rows), jnp.int32),
                pltpu.VMEM((picks, rows), F32),
                pltpu.VMEM((n_tp, 1, shard), F32),
                pltpu.VMEM((length * heads, width), BF16),
                pltpu.VMEM((length * heads, width), BF16),
                pltpu.VMEM((length * heads, value_width), BF16),
                pltpu.VMEM((1, value_width), F32),
                pltpu.VMEM(gate_weight.shape, BF16),
                pltpu.VMEM(up_weight.shape, BF16),
                pltpu.VMEM(down_weight.shape, BF16),
                pltpu.VMEM((nz, rows, shard), BF16),
                pltpu.VMEM((nz, n_ep, block, shard), BF16),
                pltpu.VMEM((n_tp, n_ep, block, shard), BF16),
                pltpu.VMEM((local, count, CORES * shard), BF16),
                pltpu.VMEM((local, count, shard), F32),
                pltpu.VMEM((local, count, units), F32),
                pltpu.VMEM((local, count, units), F32),
                pltpu.VMEM((local, count, units), BF16),
                pltpu.VMEM((CORES, nz, local, count, shard), BF16),
                pltpu.VMEM((nz, local, count, shard), BF16),
                pltpu.VMEM((nz, n_ep, block, shard), BF16),
                pltpu.VMEM((nz, n_ep, block, shard), BF16),
                pltpu.VMEM((2, n_ep, block, shard), BF16),
                pltpu.VMEM((nz, rows, shard), BF16),
                pltpu.VMEM((nz, rows, shard), BF16),
                pltpu.VMEM((rows, shard), F32),
                pltpu.VMEM((n_ep, block, shard), BF16),
                pltpu.VMEM((n_ep, block, shard), BF16),
                pltpu.VMEM((picks, rows, n_ep * block), BF16),
                pltpu.VMEM((picks, rows, 128), F32),
                pltpu.VMEM((2 * heads, length, width), BF16),
                pltpu.VMEM((2, heads, length, width), BF16),
                pltpu.VMEM((n_ep, 2, heads, length, width), BF16),
                pltpu.VMEM((2 * heads, length, LANES), F32),
                pltpu.VMEM((2 * heads, length, LANES), F32),
                pltpu.VMEM((2 * heads, length, value_width), F32),
                dma((8,)),
                dma((3,)),
                dma((2, nz - 1)), dma((2, nz - 1)),
                dma((nz, peers)), dma((nz, peers)),
                dma((nz, n_ep)), dma((nz, n_ep)),
                dma((max(peers, 2),)), dma((n_ep,)),
                dma((2, 2)), dma((2, 2)),
                dma((2,)), dma((2,)),
                dma((nz,)), dma((nz,)),
                dma((nz, peers)), dma((nz, peers)),
                dma((2,)), dma((2,)),
                dma((nz,)), dma((nz,)),
                dma((peers,)), dma((peers,)),
            ],
            compiler_params=pltpu.CompilerParams(
                collective_id=0, has_side_effects=True, vmem_limit_bytes=54 * 2**20),
            name="layer",
        )(*(pltpu.with_memory_space_constraint(x, pltpu.HBM) for x in (
            tokens, jnp.transpose(routes), jnp.transpose(route_weights),
            expert_gain.reshape(n_tp, 1, shard), gate_weight, up_weight, down_weight,
            queries.reshape(length * heads, width), keys.reshape(length * heads, width),
            values.reshape(length * heads, value_width), sub_gain[None, :],
        )), mix_weight)
        attn, moe = pl.pallas_call(
            store_kernel,
            out_shape=(
                jax.ShapeDtypeStruct((length * heads, value_width), BF16),
                jax.ShapeDtypeStruct((rows, shard), BF16),
            ),
            in_specs=[vmem, vmem],
            out_specs=(hbm, hbm),
            scratch_shapes=[dma((2,))],
            compiler_params=pltpu.CompilerParams(vmem_limit_bytes=4 * 2**20),
            name="store",
        )(attn, moe)
        return attn.reshape(length, heads, value_width), moe

    return shards


def solution(mesh):
    return jax.shard_map(
        make_shards(mesh.shape["ep"], mesh.shape["tp"]),
        mesh=mesh,
        in_specs=(
            P("ep", "tp", None),
            P("ep", "tp", None),
            P("ep", "tp", None),
            P("tp"),
            P(),
            P("ep", "tp"),
            P("ep", None),
            P("ep", None),
            P(),
            P("ep", None, "tp"),
            P("ep", None, "tp"),
            P("ep", "tp", None),
        ),
        out_specs=(P("ep", "tp", None), P("ep", "tp")),
        check_vma=False,
    )
```

```python
import functools

import jax
import jax.numpy as jnp
from jax import lax
from jax.experimental import pallas as pl
from jax.experimental.pallas import tpu as pltpu
from jax.sharding import PartitionSpec as P

NEG_FILL = -1e30
SUB_EPS = 1e-05
NORM_EPS = 1e-06
CLAMP_LIMIT = 7.0
GLU_ALPHA = 1.702
OUT_SCALE = 0.8
CORES = 2
LANES = 128
F32 = jnp.float32
BF16 = jnp.bfloat16
MESH = pl.DeviceIdType.MESH


def dot(a, b):
    return jnp.dot(a, b, preferred_element_type=F32)


def dot_t(a, b):
    return lax.dot_general(a, b, (((1,), (1,)), ((), ())), preferred_element_type=F32)


def loop(lower, upper, body):
    def step(index, carry):
        body(index)
        return carry

    lax.fori_loop(lower, upper, step, 0)


def layer_kernel(
    n_ep, n_tp, cap, heads, rank_pad,
    tok_hbm, routes_hbm, route_w_hbm, gain_hbm, gate_hbm, up_hbm, down_hbm,
    q_hbm, k_hbm, v_hbm, sub_gain_hbm, mix_hbm,
    attn_out, moe_out,
    tok, routes_t, route_w_t, gain, q_in, k_in, v_in, sub_gain, mix,
    gate, up, down, held, outgoing, arrived, normed, squares, gate_sum, up_sum, hidden, part, pair,
    fin, ex, slot_got, tok_stage, tok_got, held_sum, final, back, pick, pick_w, q, kv, kv_all,
    top, norm_sum, weighted,
    in_sem, w_sem, ag_s, ag_r, dp_s, dp_r, fw_s, fw_r, kv_s, kv_r, kh_s, kh_r, kq_s, kq_r, pr_s, pr_r,
    ex_s, ex_r, sl_s, sl_r, tk_s, tk_r, rt_s, rt_r,
):
    e, t = lax.axis_index("ep"), lax.axis_index("tp")
    nz = n_tp // CORES
    z, c = t // CORES, t % CORES
    partner = t + 1 - 2 * c
    rows, shard = tok.shape
    local = gate_hbm.shape[0]
    experts = n_ep * local
    pad = rank_pad
    slots = experts * pad
    block = local * pad
    has_up, has_dn = z < nz - 1, z > 0

    loads = [
        pltpu.make_async_copy(source, target, in_sem.at[i])
        for i, (source, target) in enumerate((
            (tok_hbm, tok), (routes_hbm, routes_t), (route_w_hbm, route_w_t), (gain_hbm, gain),
            (q_hbm, q_in), (k_hbm, k_in), (v_hbm, v_in), (sub_gain_hbm, sub_gain), (mix_hbm, mix)))
    ]
    for copy in loads:
        copy.start()
    weights = [
        pltpu.make_async_copy(source, target, w_sem.at[i])
        for i, (source, target) in enumerate(((gate_hbm, gate), (up_hbm, up), (down_hbm, down)))
    ]
    for copy in weights:
        copy.start()

    barrier = pltpu.get_barrier_semaphore()
    pl.semaphore_signal(barrier, inc=1, device_id=(e, partner), device_id_type=MESH)

    @pl.when(has_up)
    def _():
        pl.semaphore_signal(barrier, inc=1, device_id=(e, t + CORES), device_id_type=MESH)

    @pl.when(has_dn)
    def _():
        pl.semaphore_signal(barrier, inc=1, device_id=(e, t - CORES), device_id_type=MESH)

    loop(1, n_ep, lambda d: pl.semaphore_signal(
        barrier, inc=1, device_id=((e + d) % n_ep, t), device_id_type=MESH))
    for copy in loads[:2]:
        copy.wait()
    with jax.named_scope("barrier"):
        pl.semaphore_wait(barrier, n_ep + has_up.astype(jnp.int32) + has_dn.astype(jnp.int32))

    def send(source, target, s_sem, r_sem, device):
        return pltpu.make_async_remote_copy(
            src_ref=source, dst_ref=target, send_sem=s_sem, recv_sem=r_sem,
            device_id=device, device_id_type=MESH)

    def shard_copy(way, r, origin):
        source = tok if r == 0 else held.at[origin]
        target = t + CORES if way == 0 else t - CORES
        return send(source, held.at[origin], ag_s.at[way, r], ag_r.at[way, r], (e, target))

    def shard_sends(r):
        @pl.when(has_up & (z - r >= 0))
        def _():
            shard_copy(0, r, z - r).start()

        @pl.when(has_dn & (z + r < nz))
        def _():
            shard_copy(1, r, z + r).start()

    def shard_send_waits(r):
        @pl.when(has_up & (z - r >= 0))
        def _():
            shard_copy(0, r, z - r).wait_send()

        @pl.when(has_dn & (z + r < nz))
        def _():
            shard_copy(1, r, z + r).wait_send()

    shard_sends(0)

    row_i = lax.broadcasted_iota(jnp.int32, (rows, rows), 0)
    col_i = lax.broadcasted_iota(jnp.int32, (rows, rows), 1)
    picks = routes_t.shape[0]
    exp_row = lax.broadcasted_iota(jnp.int32, (experts, rows), 0)
    hot_t = [(routes_t[p:p + 1, :] == exp_row).astype(F32) for p in range(picks)]
    before_t = dot(sum(hot_t).astype(BF16), (row_i < col_i).astype(F32).astype(BF16))
    slot_row = [
        jnp.sum(h * (before_t + (exp_row * pad).astype(F32)), axis=0, keepdims=True)
        for h in hot_t
    ]
    slot_i = lax.broadcasted_iota(jnp.int32, (slots, rows), 0).astype(F32)

    def as_column(line):
        return jnp.transpose(jnp.broadcast_to(line, (128, rows)))[:, :1]

    choose = sum((slot_i == s).astype(F32) for s in slot_row).astype(BF16)

    def piece(k, d):
        source = outgoing.at[k, (e + d) % n_ep]
        return send(source, arrived.at[CORES * k + c, e], dp_s.at[k, d - 1], dp_r.at[k, d - 1],
                    ((e + d) % n_ep, t))

    def incoming(k, d):
        origin = (e + n_ep - d) % n_ep
        return send(outgoing.at[k, origin], arrived.at[CORES * k + c, origin],
                    dp_s.at[k, d - 1], dp_r.at[k, d - 1], (origin, t))

    def forward(k, d):
        origin = (e + n_ep - d) % n_ep
        place = arrived.at[CORES * k + c, origin]
        return send(place, place, fw_s.at[k, d], fw_r.at[k, d], (e, partner))

    def forwarded(k, d):
        origin = (e + n_ep - d) % n_ep
        place = arrived.at[CORES * k + 1 - c, origin]
        return send(place, place, fw_s.at[k, d], fw_r.at[k, d], (e, partner))

    def dispatch(k, source):
        made = dot(choose, source).astype(BF16).reshape(n_ep, block, shard)
        outgoing[k] = made
        arrived[CORES * k + c, e] = outgoing[k, e]
        loop(1, n_ep, lambda d: piece(k, d).start())
        forward(k, 0).start()

    items, width = q.shape[1:]

    def unpack():
        for copy in loads[2:]:
            copy.wait()
        pick_i = lax.broadcasted_iota(jnp.int32, (items, items * heads), 0)
        from_i = lax.broadcasted_iota(jnp.int32, (items, items * heads), 1)
        for h in range(heads):
            take = (from_i == pick_i * heads + h).astype(F32).astype(BF16)
            scaled_q = dot(take, q_in[...]) * (width // 2) ** -0.5
            lane = lax.broadcasted_iota(jnp.int32, (items, width), 1)
            for m in range(2):
                mine = (lane < width // 2) if m == 0 else (lane >= width // 2)
                q[2 * h + m] = jnp.where(mine, scaled_q, 0.0).astype(BF16)
            kv[0, h] = dot(take, k_in[...]).astype(BF16)
            kv[1, h] = dot(take, v_in[...]).astype(BF16)

    def pick_tables():
        lane_slot = lax.broadcasted_iota(jnp.int32, (rows, slots), 1).astype(F32)
        for p in range(picks):
            pick[p] = (lane_slot == as_column(slot_row[p])).astype(F32).astype(BF16)
            pick_w[p] = jnp.transpose(jnp.broadcast_to(route_w_t[p:p + 1, :], (128, rows)))

    length = items
    value_width = kv.shape[3]
    ones = jnp.ones((length, LANES), BF16)

    def across(column, lanes):
        return jnp.concatenate([column] * (lanes // LANES), axis=1)

    def attend(keys_values, diagonal):
        for h in range(heads):
            key = keys_values[0, h]
            value = jnp.concatenate([keys_values[1, h], ones], axis=1)
            for m in range(2):
                n = 2 * h + m
                scores = dot_t(q[n], key)
                if diagonal:
                    q_pos = lax.broadcasted_iota(jnp.int32, scores.shape, 0)
                    k_pos = lax.broadcasted_iota(jnp.int32, scores.shape, 1)
                    scores = jnp.where(k_pos <= q_pos, scores, NEG_FILL)
                high = jnp.max(scores, axis=1, keepdims=True)
                if diagonal:
                    high = jnp.broadcast_to(high, (length, LANES))
                else:
                    old = top[n]
                    high = jnp.maximum(high, old)
                    shrink = jnp.exp(old - high)
                w = jnp.exp(scores - across(high, length)).astype(BF16)
                both = dot(w, value)
                v, s = both[:, :value_width], both[:, value_width:]
                top[n] = high
                norm_sum[n] = s if diagonal else norm_sum[n] * shrink + s
                weighted[n] = v if diagonal else weighted[n] * across(shrink, value_width) + v

    relay = n_ep == 4

    def kv_copy(d):
        return send(kv, kv_all.at[e], kv_s.at[d - 1], kv_r.at[e], ((e + d) % n_ep, t))

    def kv_got(origin):
        return send(kv, kv_all.at[origin], kv_s.at[0], kv_r.at[origin], (origin, t))

    def kv_half(origin, half, device, own=False):
        place = kv_all.at[origin, half]
        return send(kv.at[half] if own else place, place, kh_s.at[origin, half],
                    kh_r.at[origin, half], (device, t))

    def kv_early(action):
        if relay:
            @pl.when(e % 2 == 0)
            def _():
                action(kv_copy(1))

            @pl.when(e == 1)
            def _():
                action(kv_copy(2))
        else:
            loop(1, n_ep - e, lambda d: action(kv_copy(d)))

    def kv_middle(action):
        if relay:
            @pl.when(e == 0)
            def _():
                action(kv_half(0, 1, 2, True))

    def kv_late(action):
        if relay:
            @pl.when(e == 0)
            def _():
                action(kv_half(0, 0, 2, True))

            if near:
                @pl.when(e == 1)
                def _():
                    action(kv_heads(True))

    def kv_second(action):
        if relay:
            @pl.when(e == 2)
            def _():
                action(kv_half(0, 1, 3))

    near = heads // 2

    def kv_heads(own):
        span = pl.ds(0, near) if own else pl.ds(near, heads - near)
        place = kv_all.at[1, 1, span]
        index = 0 if own else 1
        return send(kv.at[1, span] if own else place, place, kq_s.at[index], kq_r.at[index], (2, t))

    def kv_pass(origin, action):
        if relay:
            @pl.when((e == 1) & (origin == 0))
            def _():
                action(kv_half(0, 0, 3))

            @pl.when((e == 3) & (origin == 1))
            def _():
                action(kv_half(1, 0, 2))
                action(kv_heads(False))

    def far_origin(j):
        if relay:
            return jnp.where(e == 3, (j + 1) % 3, j)
        return e - 1 - j

    def attend_far(lower, upper):
        def body(j):
            origin = far_origin(j)
            if relay:
                halves = (e == 2) | ((e == 3) & (origin == 0))

                @pl.when(halves)
                def _():
                    kv_half(origin, 0, 3).wait_recv()

                @pl.when(halves & (e == 3))
                def _():
                    kv_half(origin, 1, 3).wait_recv()

                @pl.when(halves & (e == 2) & (origin == 1))
                def _():
                    kv_heads(False).wait_recv()
                    if near:
                        kv_heads(True).wait_recv()

                @pl.when(jnp.logical_not(halves))
                def _():
                    kv_got(origin).wait_recv()
            else:
                kv_got(origin).wait_recv()
            kv_pass(origin, lambda copy: copy.start())
            attend(kv_all.at[origin], False)

        loop(lower, jnp.minimum(upper, e), body)

    with jax.named_scope("dispatch_own"):
        dispatch(z, tok[...])
    with jax.named_scope("unpack"):
        unpack()
    for r in range(nz - 1):
        got_up = has_dn & (z - 1 - r >= 0)
        got_dn = has_up & (z + 1 + r < nz)

        with jax.named_scope("shard_wait"):
            @pl.when(got_up)
            def _():
                shard_copy(0, r, z - 1 - r).wait_recv()

            @pl.when(got_dn)
            def _():
                shard_copy(1, r, z + 1 + r).wait_recv()

            if r < nz - 2:
                shard_sends(r + 1)

        with jax.named_scope("dispatch"):
            @pl.when(got_up)
            def _():
                dispatch(z - 1 - r, held[z - 1 - r])

            @pl.when(got_dn)
            def _():
                dispatch(z + 1 + r, held[z + 1 + r])

        if r == 0:
            with jax.named_scope("diag"):
                attend(kv, True)
                pick_tables()

    kv_early(lambda copy: copy.start())

    def pass_on(k):
        def body(d):
            incoming(k, d).wait_recv()
            forward(k, d).start()

        loop(1, n_ep, body)

    for copy in weights:
        copy.wait()
    gate_sum[...] = jnp.zeros_like(gate_sum)
    up_sum[...] = jnp.zeros_like(up_sum)
    squares[...] = jnp.zeros_like(squares)
    width_total = gain.shape[2] * n_tp
    deep = CORES * shard

    def absorb(k):
        loop(0, n_ep, lambda d: forwarded(k, d).wait_recv())

        def prepare(source):
            place = pl.ds(pl.multiple_of(source * pad, pad), pad)
            for x in range(local):
                for half in range(CORES):
                    floats = arrived[CORES * k + half, source, x * pad:(x + 1) * pad, :].astype(F32)
                    squares[x, place, :] += floats * floats
                    normed[x, place, half * shard:(half + 1) * shard] = (
                        floats * gain[CORES * k + half]).astype(BF16)

        loop(0, n_ep, prepare)
        depth = pl.ds(pl.multiple_of(k * deep, deep), deep)
        for x in range(local):
            gate_sum[x] += dot(normed[x], gate[x, depth, :])
            up_sum[x] += dot(normed[x], up[x, depth, :])

    def visit(i, action):
        k = z - (i + 1) // 2 * (i % 2) + i // 2 * (1 - i % 2)

        @pl.when((k >= 0) & (k < nz))
        def _():
            action(k)

    def arrival(i):
        @pl.when(i < 2 * nz - 1)
        def _():
            visit(i, pass_on)

        @pl.when(i == 2 * nz - 2)
        def _():
            kv_middle(lambda copy: copy.start())

        @pl.when(i >= 2)
        def _():
            visit(i - 2, absorb)

    with jax.named_scope("absorb"):
        loop(0, 2 * nz + 1, arrival)

    count = n_ep * pad

    def goal(i):
        down, up_to = nz - 1 - i, i
        down = jnp.where(down <= z, down - 1, down)
        up_to = jnp.where(up_to >= z, up_to + 1, up_to)
        return jnp.where(i == nz - 1, z, jnp.where(2 * z < nz, down, up_to))

    def pair_copy(k):
        return send(part.at[1 - c, k], pair.at[k], pr_s.at[k], pr_r.at[k], (e, partner))

    def exchange(k, d):
        target = (e + d) % n_ep
        return send(fin.at[k, target], ex.at[k, e], ex_s.at[k, d - 1], ex_r.at[k, d - 1], (target, t))

    def exchanged(k, d):
        origin = (e + n_ep - d) % n_ep
        return send(fin.at[k, origin], ex.at[k, origin], ex_s.at[k, d - 1], ex_r.at[k, d - 1],
                    (origin, t))

    def slot_copy(way):
        k = z + 1 if way == 0 else z - 1
        target = t + CORES if way == 0 else t - CORES
        return send(fin.at[k], slot_got.at[way], sl_s.at[way], sl_r.at[way], (e, target))

    def slot_recv(way):
        return send(fin.at[z], slot_got.at[way], sl_s.at[way], sl_r.at[way], (e, partner))

    def token_copy(k):
        return send(tok_stage.at[k], tok_got.at[z], tk_s.at[k], tk_r.at[z], (e, CORES * k + c))

    def token_got(k):
        return send(tok_stage.at[k], tok_got.at[k], tk_s.at[k], tk_r.at[k], (e, CORES * k + c))

    def is_far(k):
        return (k > z + 1) | (k < z - 1)

    with jax.named_scope("hidden"):
        for x in range(local):
            mean = jnp.sum(squares[x], axis=1, keepdims=True) / width_total
            factor = lax.rsqrt(mean + NORM_EPS)
            gate_pre = jnp.minimum(gate_sum[x] * factor, CLAMP_LIMIT)
            up_pre = jnp.clip(up_sum[x] * factor, -CLAMP_LIMIT, CLAMP_LIMIT)
            hidden[x] = ((up_pre + 1.0) * gate_pre * jax.nn.sigmoid(GLU_ALPHA * gate_pre)).astype(BF16)

    def project(i):
        k = goal(i)
        place = pl.ds(pl.multiple_of(k * deep, deep), deep)
        for x in range(local):
            product = dot(hidden[x], down[x, :, place]).astype(BF16)
            for half in range(CORES):
                part[half, k, x] = product[:, half * shard:(half + 1) * shard]
        pair_copy(k).start()

    def finish(i):
        k = goal(i)
        pair_copy(k).wait_recv()
        for x in range(local):
            both = (part[c, k, x].astype(F32) + pair[k, x].astype(F32)).astype(BF16)
            for source in range(n_ep):
                fin[k, source, x * pad:(x + 1) * pad, :] = both[source * pad:(source + 1) * pad, :]

        @pl.when(is_far(k))
        def _():
            loop(1, n_ep, lambda d: exchange(k, d).start())

        @pl.when(k == z + 1)
        def _():
            slot_copy(0).start()

        @pl.when(k == z - 1)
        def _():
            slot_copy(1).start()

    def step(i):
        @pl.when(i < nz)
        def _():
            project(i)

        @pl.when(i >= 2)
        def _():
            finish(i - 2)

    with jax.named_scope("finish"):
        loop(0, nz + 2, step)
        kv_late(lambda copy: copy.start())

    def mixture(results):
        mixed = None
        for p in range(picks):
            selected = dot(pick[p], results)
            weight = jnp.concatenate([pick_w[p]] * (shard // 128), axis=1)
            mixed = selected * weight if mixed is None else mixed + selected * weight
        return mixed

    def tokens_out(i):
        k = goal(i)

        @pl.when(is_far(k))
        def _():
            ex[k, e] = fin[k, e]
            loop(1, n_ep, lambda d: exchanged(k, d).wait_recv())
            tok_stage[k] = mixture(ex[k].reshape(slots, shard)).astype(BF16)
            token_copy(k).start()

    early = jnp.where(e == 2, 0, e) if relay else 0
    early = jnp.minimum(early, 2)
    with jax.named_scope("second"):
        if relay:
            @pl.when(e == 2)
            def _():
                kv_half(0, 1, 3).wait_recv()
                kv_half(0, 1, 3).start()
    with jax.named_scope("far0"):
        attend_far(0, early)
    with jax.named_scope("tokens_out"):
        loop(0, nz, tokens_out)
    with jax.named_scope("slots_in"):
        @pl.when(has_dn)
        def _():
            slot_recv(0).wait_recv()

        @pl.when(has_up)
        def _():
            slot_recv(1).wait_recv()

        for x in range(local):
            span = slice(x * pad, (x + 1) * pad)
            for source in range(n_ep):
                total = fin[z, source, span, :].astype(F32)
                low = slot_got[0, source, span, :].astype(F32)
                high = slot_got[1, source, span, :].astype(F32)
                total = total + jnp.where(has_dn, low, 0.0) + jnp.where(has_up, high, 0.0)
                final[source, span, :] = total.astype(BF16)

    def give(d):
        return send(final.at[(e + d) % n_ep], back.at[e], rt_s.at[d - 1], rt_r.at[d - 1],
                    ((e + d) % n_ep, t))

    def given(d):
        origin = (e + n_ep - d) % n_ep
        return send(final.at[origin], back.at[origin], rt_s.at[d - 1], rt_r.at[d - 1], (origin, t))

    loop(1, n_ep, lambda d: give(d).start())
    back[e] = final[e]

    with jax.named_scope("early_waits"):
        for r in range(nz - 1):
            shard_send_waits(r)
        loop(0, nz, lambda k: loop(1, n_ep, lambda d: piece(k, d).wait_send()))
        loop(0, nz, lambda k: loop(0, n_ep, lambda d: forward(k, d).wait_send()))
        loop(0, nz, lambda k: pair_copy(k).wait_send())

    with jax.named_scope("far2"):
        attend_far(early, n_ep)
    with jax.named_scope("attn_fin"):
        finished = []
        for h in range(heads):
            first, second = (
                weighted[n] / across(norm_sum[n], value_width) for n in (2 * h, 2 * h + 1))
            blend = first - mix[h] * second
            mean = jnp.mean(blend * blend, axis=1, keepdims=True)
            scaled = (blend * lax.rsqrt(mean + SUB_EPS) * sub_gain[...] * OUT_SCALE).astype(BF16)
            finished.append(scaled)
        put_i = lax.broadcasted_iota(jnp.int32, (items * heads, items), 0)
        of_i = lax.broadcasted_iota(jnp.int32, (items * heads, items), 1)
        spread = (put_i // heads == of_i).astype(F32).astype(BF16)
        wide = dot(spread, jnp.concatenate(finished, axis=1))
        head_i = lax.broadcasted_iota(jnp.int32, (items * heads, value_width), 0) % heads
        woven = wide[:, :value_width]
        for h in range(1, heads):
            woven = jnp.where(head_i == h, wide[:, h * value_width:(h + 1) * value_width], woven)
        attn_out[...] = woven.astype(BF16)

    with jax.named_scope("tokens_in"):
        held_sum[...] = jnp.zeros_like(held_sum)

        def add_far(k):
            @pl.when(is_far(k))
            def _():
                token_got(k).wait_recv()
                held_sum[...] += tok_got[k].astype(F32)

        loop(0, nz, add_far)

    with jax.named_scope("given_wait"):
        loop(1, n_ep, lambda d: given(d).wait_recv())
    with jax.named_scope("combine"):
        moe_out[...] = (mixture(back[...].reshape(slots, shard)) + held_sum[...]).astype(BF16)
        def far_waits(k):
            @pl.when(is_far(k))
            def _():
                loop(1, n_ep, lambda d: exchange(k, d).wait_send())
                token_copy(k).wait_send()

        loop(0, nz, far_waits)

        @pl.when(has_up)
        def _():
            slot_copy(0).wait_send()

        @pl.when(has_dn)
        def _():
            slot_copy(1).wait_send()

        loop(1, n_ep, lambda d: give(d).wait_send())
        for part_of in (kv_early, kv_middle, kv_late, kv_second):
            part_of(lambda copy: copy.wait_send())
        if relay:
            for origin in range(2):
                kv_pass(origin, lambda copy: copy.wait_send())


def store_kernel(attn, moe, attn_hbm, moe_hbm, sems):
    copies = [
        pltpu.make_async_copy(source, target, sems.at[i])
        for i, (source, target) in enumerate(((attn, attn_hbm), (moe, moe_hbm)))
    ]
    for copy in copies:
        copy.start()
    for copy in copies:
        copy.wait()


def make_shards(n_ep, n_tp):
    def shards(
        queries, keys, values, mix_weight, sub_gain, tokens, routes, route_weights,
        expert_gain, gate_weight, up_weight, down_weight,
    ):
        rows, shard = tokens.shape
        picks = routes.shape[1]
        local, depth, units = gate_weight.shape
        cap = 3 * rows * picks // (2 * n_ep * local)
        pad = -(-cap // 16) * 16
        length, heads, width = queries.shape
        value_width = values.shape[2]
        nz = n_tp // CORES
        block = local * pad
        count = n_ep * pad
        vmem = pl.BlockSpec(memory_space=pltpu.VMEM)
        hbm = pl.BlockSpec(memory_space=pltpu.HBM)
        dma = pltpu.SemaphoreType.DMA
        peers = n_ep - 1
        attn, moe = pl.pallas_call(
            functools.partial(layer_kernel, n_ep, n_tp, cap, heads, pad),
            out_shape=(
                pltpu.VMEM((length * heads, value_width), BF16),
                pltpu.VMEM((rows, shard), BF16),
            ),
            in_specs=[hbm] * 12,
            out_specs=(vmem, vmem),
            scratch_shapes=[
                pltpu.VMEM((rows, shard), BF16),
                pltpu.VMEM((picks, rows), jnp.int32),
                pltpu.VMEM((picks, rows), F32),
                pltpu.VMEM((n_tp, 1, shard), F32),
                pltpu.VMEM((length * heads, width), BF16),
                pltpu.VMEM((length * heads, width), BF16),
                pltpu.VMEM((length * heads, value_width), BF16),
                pltpu.VMEM((1, value_width), F32),
                pltpu.SMEM((heads,), F32),
                pltpu.VMEM(gate_weight.shape, BF16),
                pltpu.VMEM(up_weight.shape, BF16),
                pltpu.VMEM(down_weight.shape, BF16),
                pltpu.VMEM((nz, rows, shard), BF16),
                pltpu.VMEM((nz, n_ep, block, shard), BF16),
                pltpu.VMEM((n_tp, n_ep, block, shard), BF16),
                pltpu.VMEM((local, count, CORES * shard), BF16),
                pltpu.VMEM((local, count, shard), F32),
                pltpu.VMEM((local, count, units), F32),
                pltpu.VMEM((local, count, units), F32),
                pltpu.VMEM((local, count, units), BF16),
                pltpu.VMEM((CORES, nz, local, count, shard), BF16),
                pltpu.VMEM((nz, local, count, shard), BF16),
                pltpu.VMEM((nz, n_ep, block, shard), BF16),
                pltpu.VMEM((nz, n_ep, block, shard), BF16),
                pltpu.VMEM((2, n_ep, block, shard), BF16),
                pltpu.VMEM((nz, rows, shard), BF16),
                pltpu.VMEM((nz, rows, shard), BF16),
                pltpu.VMEM((rows, shard), F32),
                pltpu.VMEM((n_ep, block, shard), BF16),
                pltpu.VMEM((n_ep, block, shard), BF16),
                pltpu.VMEM((picks, rows, n_ep * block), BF16),
                pltpu.VMEM((picks, rows, 128), F32),
                pltpu.VMEM((2 * heads, length, width), BF16),
                pltpu.VMEM((2, heads, length, width), BF16),
                pltpu.VMEM((n_ep, 2, heads, length, width), BF16),
                pltpu.VMEM((2 * heads, length, LANES), F32),
                pltpu.VMEM((2 * heads, length, LANES), F32),
                pltpu.VMEM((2 * heads, length, value_width), F32),
                dma((9,)),
                dma((3,)),
                dma((2, nz - 1)), dma((2, nz - 1)),
                dma((nz, peers)), dma((nz, peers)),
                dma((nz, n_ep)), dma((nz, n_ep)),
                dma((max(peers, 2),)), dma((n_ep,)),
                dma((2, 2)), dma((2, 2)),
                dma((2,)), dma((2,)),
                dma((nz,)), dma((nz,)),
                dma((nz, peers)), dma((nz, peers)),
                dma((2,)), dma((2,)),
                dma((nz,)), dma((nz,)),
                dma((peers,)), dma((peers,)),
            ],
            compiler_params=pltpu.CompilerParams(
                collective_id=0, has_side_effects=True, vmem_limit_bytes=54 * 2**20),
            name="layer",
        )(*(pltpu.with_memory_space_constraint(x, pltpu.HBM) for x in (
            tokens, jnp.transpose(routes), jnp.transpose(route_weights),
            expert_gain.reshape(n_tp, 1, shard), gate_weight, up_weight, down_weight,
            queries.reshape(length * heads, width), keys.reshape(length * heads, width),
            values.reshape(length * heads, value_width), sub_gain[None, :],
        )), pltpu.with_memory_space_constraint(mix_weight, pltpu.HBM) if heads > 1 else mix_weight)
        attn, moe = pl.pallas_call(
            store_kernel,
            out_shape=(
                jax.ShapeDtypeStruct((length * heads, value_width), BF16),
                jax.ShapeDtypeStruct((rows, shard), BF16),
            ),
            in_specs=[vmem, vmem],
            out_specs=(hbm, hbm),
            scratch_shapes=[dma((2,))],
            compiler_params=pltpu.CompilerParams(vmem_limit_bytes=4 * 2**20),
            name="store",
        )(attn, moe)
        return attn.reshape(length, heads, value_width), moe

    return shards


def solution(mesh):
    return jax.shard_map(
        make_shards(mesh.shape["ep"], mesh.shape["tp"]),
        mesh=mesh,
        in_specs=(
            P("ep", "tp", None),
            P("ep", "tp", None),
            P("ep", "tp", None),
            P("tp"),
            P(),
            P("ep", "tp"),
            P("ep", None),
            P("ep", None),
            P(),
            P("ep", None, "tp"),
            P("ep", None, "tp"),
            P("ep", "tp", None),
        ),
        out_specs=(P("ep", "tp", None), P("ep", "tp")),
        check_vma=False,
    )
```
